128 devices in a mesh: ep: 128 (over z, y, x, core).
Axes of the slice: x: 4, y: 4, z: 4, core: 2. Of those that a mesh axis runs over, the one named last changes fastest.
Arguments:
- tokens: bfloat16 [16384, 2048], P('ep'), may hold values from -6 to 6
- norm_gain: float32 [2048], replicated, may hold values from 0.1 to 1.9
- route_ids: int32 [16384, 2], P('ep'), may hold values from 0 to 127, all different within a row; in each aligned block of 128 rows (0 to 127, 128 to 255, ...) at most 8 rows name the same one
- route_weight: float32 [16384, 2], P('ep'), may hold values from 0.25 to 1
- expert_gate: bfloat16 [128, 2048, 1024], P('ep'), may hold values from -0.125 to 0.125
- expert_up: bfloat16 [128, 2048, 1024], P('ep'), may hold values from -0.125 to 0.125
- expert_down: bfloat16 [128, 1024, 2048], P('ep'), may hold values from -0.1875 to 0.1875
- dense_up: bfloat16 [2048, 512], P('ep'), may hold values from -0.125 to 0.125
- dense_down: bfloat16 [512, 2048], P(None, 'ep'), may hold values from -0.25 to 0.25
- branch_gate: float32 [2048], replicated, may hold values from -1.5 to 1.5
Outputs:
- mixed: bfloat16 [16384, 2048], P('ep')
The draws below stay inside these ranges and needn't reach their ends.
Inputs may be any that keep to these rules, and one draw needn't show every extreme that they name: `route_ids`: each token names 2 different experts; among the 128 tokens of one device (aligned blocks of rows) no expert is named more than 8 times, and in every draw some expert is named exactly 8 times by some device's tokens; every expert is named by some token.
All inputs are finite; a program needn't handle non-finite values.
Results may differ from the reference program's by a relative error of at most 0.01.
Values may be sent and summed in bfloat16 or wider, within the bound.
A program may use at most 128 MiB of HBM per device.

```python
import math
import jax
import jax.numpy as jnp
import numpy as np
from jax import lax

D = 2048
FF = 1024
DH = 512
TOP = 2
CAP = 8
TOK_DEV = 128
TOKENS = 16384
EXPERTS = 128
N_EP = 128


def steps_of(key, extent, split, smallest, top_value):
    def one(dim, blocks):
        heights = jax.random.uniform(jax.random.fold_in(jax.random.fold_in(key, 6), dim), (blocks,), jnp.float32, smallest / len(split), top_value / len(split))
        return jnp.repeat(jnp.exp(heights), extent[dim] // blocks).reshape((-1,) + (1,) * (len(extent) - dim - 1))

    level = one(*split[0])
    for cut in split[1:]:
        level = level * one(*cut)
    return level


def shared_out(own_key, own, number, rows, count, top, limit, lean):
    ranking = jax.random.permutation(own_key, count)
    crowded, common = load_shares(count, rows * top, limit, lean, True), load_shares(count, rows * top, limit, lean, False)
    places = jnp.arange(count)

    def named(sizes, rotation):
        used = int((sizes > 0).sum())
        fixed = max(1, used // 4)
        moved = fixed + (places - fixed + rotation * (used - fixed)) % max(1, count - fixed)
        return jnp.zeros((count,), jnp.int32).at[ranking[jnp.where(places < fixed, places, moved)]].set(jnp.asarray(sizes, jnp.int32))

    sizes = jnp.where(number % 4 == 0, named(crowded, number // 4), named(common, number - number // 4 - 1))
    mixed = jax.random.permutation(jax.random.fold_in(own, 3), count)
    source_of, taker = mixed[0:count // 2 * 2:2], mixed[1:count // 2 * 2:2]
    slack = jnp.minimum(sizes[source_of] - 1, limit - sizes[taker]) // 2
    slack = jnp.where((source_of == ranking[0]) | (taker == ranking[0]) | (sizes[taker] == 0), 0, jnp.maximum(slack, 0))
    moved = jax.random.randint(jax.random.fold_in(own, 4), (count // 2,), 0, 1 << 20) % (slack + 1)
    sizes = sizes.at[source_of].add(-moved).at[taker].add(moved)
    labels = jnp.searchsorted(jnp.cumsum(sizes), jnp.arange(rows * top), side="right").astype(jnp.int32)
    grid = labels.reshape(top, rows).T
    grid = grid[jax.random.permutation(jax.random.fold_in(own, 1), rows)]
    rotation = jax.random.randint(jax.random.fold_in(own, 2), (rows, 1), 0, top)
    return jnp.take_along_axis(grid, (jnp.arange(top)[None, :] + rotation) % top, axis=1)


def load_shares(count, total, bound, slope, full):
    weights = [(1 << 20) // math.isqrt(rank ** slope) + 1 for rank in range(1, count + 1)]
    largest = bound if full else min(bound, max(-(-total // count), total * weights[0] // sum(weights)))
    least = 1 if total - largest >= count - 1 else 0
    counts, spare = [largest] + [least] * (count - 1), total - largest - least * (count - 1)
    while spare > 0:
        candidates = [i for i in range(1, count) if counts[i] < largest] or [i for i in range(1, count) if counts[i] < bound]
        whole, budget = sum([weights[i] for i in candidates]), spare
        for i in candidates:
            addition = min(bound - counts[i], max(1, budget * weights[i] // whole), spare)
            counts[i] = counts[i] + addition
            spare = spare - addition
    return np.array(counts)


def scatter_about(rng, extent, deviation, reach, split=(), kind=jnp.bfloat16):
    gain = steps_of(rng, extent, split, -0.22, 0.18) if split else 1.0
    values = jax.random.normal(rng, extent, jnp.float32) * deviation * gain
    return jnp.minimum(jnp.maximum(values, -reach), reach).astype(kind)


def setup_inputs(seed: int = 0) -> dict:
    streams_of = jax.random.split(jax.random.key(seed), 11)
    tokens = scatter_about(streams_of[0], (TOKENS, D), 1.0, 6.0, ((0, 128),))
    norm_gain = jnp.clip(1.0 + 0.18 * jax.random.normal(streams_of[1], (D,), jnp.float32), 0.1, 1.9)
    route_ids_keys = jax.random.split(jax.random.fold_in(streams_of[2], 1), TOKENS // TOK_DEV)
    route_ids_turns = jax.random.permutation(jax.random.fold_in(streams_of[2], 3), TOKENS // TOK_DEV)
    route_ids = jax.vmap(lambda own, number: shared_out(jax.random.fold_in(streams_of[2], 2), own, number, TOK_DEV, EXPERTS, TOP, CAP, 2))(route_ids_keys, route_ids_turns).reshape((TOKENS, TOP))
    route_weight = jnp.clip(0.25 + 0.75 * jax.random.uniform(streams_of[3], (TOKENS, TOP), jnp.float32) ** steps_of(streams_of[3], (TOKENS, TOP), ((0, 128),), -0.2, 0.2), 0.25, 1.0)
    expert_gate = scatter_about(streams_of[4], (EXPERTS, D, FF), D ** -0.5, 0.125, ((0, 128),))
    expert_up = scatter_about(streams_of[5], (EXPERTS, D, FF), D ** -0.5, 0.125, ((0, 128),))
    expert_down = scatter_about(streams_of[6], (EXPERTS, FF, D), FF ** -0.5, 0.1875, ((0, 128),))
    dense_up = scatter_about(streams_of[7], (D, DH), D ** -0.5, 0.125, ((0, 128),))
    dense_down = scatter_about(streams_of[8], (DH, D), DH ** -0.5, 0.25, ((1, 128),))
    branch_gate = jnp.clip(jax.random.uniform(streams_of[9], (D,), jnp.float32, -1.5, 1.5), -1.5, 1.5)
    return dict(tokens=tokens, norm_gain=norm_gain, route_ids=route_ids, route_weight=route_weight, expert_gate=expert_gate, expert_up=expert_up, expert_down=expert_down, dense_up=dense_up, dense_down=dense_down, branch_gate=branch_gate)


def reference(tokens, norm_gain, route_ids, route_weight, expert_gate, expert_up, expert_down, dense_up, dense_down, branch_gate):
    wide_tokens = tokens.astype(jnp.float32)
    scale = lax.rsqrt(lax.optimization_barrier(jnp.mean(wide_tokens * wide_tokens, axis=-1, keepdims=True)) + 1e-06)
    normed = (wide_tokens * scale * norm_gain).astype(jnp.bfloat16)
    flat_ids = route_ids.reshape(-1).astype(jnp.int32)
    entries = TOKENS * TOP
    onehot = (flat_ids[:, None] == jnp.arange(EXPERTS, dtype=jnp.int32)[None, :]).astype(jnp.int32)
    blocked = onehot.reshape(N_EP, TOK_DEV * TOP, EXPERTS)
    earlier = (jnp.cumsum(blocked, axis=1) - blocked).reshape(entries, EXPERTS)
    slot_index = lax.optimization_barrier(jnp.sum(earlier * onehot, axis=-1)).astype(jnp.int32)
    source = (jnp.arange(entries, dtype=jnp.int32) // (TOK_DEV * TOP)).astype(jnp.int32)
    position = (source * CAP + slot_index).astype(jnp.int32)
    token_index = (jnp.arange(entries, dtype=jnp.int32) // TOP).astype(jnp.int32)
    table = jnp.full((EXPERTS, N_EP * CAP), TOKENS, jnp.int32).at[flat_ids, position].set(token_index)
    weight_table = jnp.zeros((EXPERTS, N_EP * CAP), jnp.float32).at[flat_ids, position].set(route_weight.reshape(-1).astype(jnp.float32))
    padded = jnp.concatenate([normed, jnp.zeros((1, D), jnp.bfloat16)], axis=0)

    def expert_step(summed, inputs):
        row_table, row_weight, w_gate, w_up, w_down = inputs
        row_block = jnp.take(padded, row_table, axis=0)
        gate_part = jnp.dot(row_block, w_gate, preferred_element_type=jnp.float32)
        up_part = jnp.dot(row_block, w_up, preferred_element_type=jnp.float32)
        hidden = (jax.nn.silu(gate_part) * up_part).astype(jnp.bfloat16)
        result = jnp.dot(hidden, w_down, preferred_element_type=jnp.float32).astype(jnp.bfloat16)
        weighted = result.astype(jnp.float32) * row_weight[:, None]
        return (summed.at[row_table].add(weighted), None)
    summed, _ = lax.scan(expert_step, jnp.zeros((TOKENS + 1, D), jnp.float32), (table, weight_table, expert_gate, expert_up, expert_down))
    combined = summed[:TOKENS]
    dense_pre = jnp.dot(normed, dense_up, preferred_element_type=jnp.float32)
    dense_hidden = jax.nn.silu(dense_pre).astype(jnp.bfloat16)
    dense_out = jnp.dot(dense_hidden, dense_down, preferred_element_type=jnp.float32)
    return (combined + jnp.tanh(branch_gate) * dense_out).astype(jnp.bfloat16)
```

```python
import functools
import itertools
import math

import jax
import jax.numpy as jnp
from jax import lax
from jax.experimental import pallas as pl
from jax.experimental.pallas import tpu as pltpu
from jax.sharding import PartitionSpec as P

CAP = 8
F32 = jnp.float32
BF16 = jnp.bfloat16


def plane_order(side, cores):
    def hop(d):
        return min(d, side - d)

    offsets = [o for o in itertools.product(range(side), range(side), range(cores)) if any(o)]
    order = []
    for o in sorted(offsets, key=lambda o: hop(o[0]) + hop(o[1])):
        for pick in (o, (-o[0] % side, -o[1] % side, o[2])):
            if pick not in order:
                order.append(pick)
    return order


def with_dim(k, d, a, b, e):
    full = [a, b]
    full.insert(k, d)
    return (*full, e)


def kernel(
    side, cores, cols,
    tokens, gain, ids, weight, w_gate, w_up, w_down, d_up, d_down, branch,
    out,
    ag, mine, info, send, recv, result, back, rs_out, rs_in, high_t, low_t, v_gate, v_up, v_down, wide,
    local_sem, info_send, info_recv, ag_send, ag_recv, out_send, out_recv, own_sem,
    ret_send, ret_recv, rs_send, rs_recv, w_send, w_recv,
):
    rows, width = tokens.shape
    plane = side * side * cores
    n = side * plane
    slots = plane * CAP
    me = lax.axis_index("ep")
    dims = (side, side, side, cores)
    strides = (plane, side * cores, cores, 1)
    at = tuple(me // strides[i] % dims[i] for i in range(4))
    part = [[(at[i] + d) % dims[i] * strides[i] for d in range(dims[i])] for i in range(4)]
    grid = (side, side, side, cores, CAP, width)
    send6, recv6, result6, back6 = (r.reshape(*grid) for r in (send, recv, result, back))
    ring = sorted(range(1, side), key=lambda d: (min(d, side - d), d))
    others = pl.ds(1, side - 1)
    order = plane_order(side, cores)
    peers = len(order)
    lanes = [pl.ds(lo, hi - lo) for lo, hi in cols]

    def dev(o):
        return part[0][o[0]] + part[1][o[1]] + part[2][o[2]] + part[3][o[3]]

    def minus(o):
        return tuple(-o[i] % dims[i] for i in range(4))

    def along(k, d):
        return tuple(d if i == k else 0 for i in range(4))

    def remote(src, dst, s, r, target):
        return pltpu.make_async_remote_copy(
            src_ref=src, dst_ref=dst, send_sem=s, recv_sem=r,
            device_id=(target,), device_id_type=pl.DeviceIdType.MESH,
        )

    near = dev((0, 0, 0, 1))

    barrier = pltpu.get_barrier_semaphore()
    greeted = sorted({with_dim(k, 0, *o) for k in range(3) for o in order})
    for o in greeted:
        pl.semaphore_signal(barrier, inc=1, device_id=(dev(o),), device_id_type=pl.DeviceIdType.MESH)

    own_up = pltpu.make_async_copy(d_up, wide.at[(0, *at)], local_sem.at[0])
    own_down = pltpu.make_async_copy(d_down, wide.at[(1, *at)], local_sem.at[1])
    own_up.start()
    own_down.start()
    loads = [
        pltpu.make_async_copy(w_gate.at[0], v_gate, local_sem.at[2]),
        pltpu.make_async_copy(w_up.at[0], v_up, local_sem.at[3]),
        pltpu.make_async_copy(w_down.at[0], v_down, local_sem.at[4]),
    ]
    for load in loads:
        load.start()

    x = tokens[...].astype(F32)
    scale = lax.rsqrt(jnp.mean(x * x, axis=-1, keepdims=True) + 1e-06)
    ag[0] = (x * scale * gain[...]).astype(BF16)
    mine[...] = jnp.concatenate(
        [ids[...].astype(F32), weight[...], jnp.zeros((4, rows), F32)], axis=0
    )

    before = lax.broadcasted_iota(jnp.int32, (rows, rows), 0) < lax.broadcasted_iota(jnp.int32, (rows, rows), 1)
    before = before.astype(F32).astype(BF16)
    j_iota = lax.broadcasted_iota(jnp.int32, (plane, rows), 0)
    p_iota = lax.broadcasted_iota(jnp.int32, (slots, rows), 0)

    def slots_of(k, facts):
        first, second = [i for i in range(3) if i != k]

        def local(expert):
            coords = [expert // strides[i] % dims[i] for i in range(4)]
            away = [(coords[i] + dims[i] - at[i]) % dims[i] for i in range(4)]
            j = (away[first] * side + away[second]) * cores + away[3]
            return jnp.where(away[k] == 0, j, -1)

        j0 = local(facts[0:1, :].astype(jnp.int32))
        j1 = local(facts[1:2, :].astype(jnp.int32))
        hot0 = (j0 == j_iota).astype(F32)
        hot1 = (j1 == j_iota).astype(F32)
        count = jnp.dot((hot0 + hot1).astype(BF16), before, preferred_element_type=F32)
        rank0 = jnp.sum(hot0 * count, axis=0, keepdims=True).astype(jnp.int32)
        rank1 = jnp.sum(hot1 * count, axis=0, keepdims=True).astype(jnp.int32)
        slot0 = jnp.where(j0 < 0, -1, j0 * CAP + rank0)
        slot1 = jnp.where(j1 < 0, -1, j1 * CAP + rank1)
        return slot0 == p_iota, slot1 == p_iota

    def pack(k, d, facts):
        lo, hi = cols[k]
        table0, table1 = slots_of(k, facts)
        place = jnp.where(table0 | table1, 1.0, 0.0).astype(BF16)
        packed = jnp.dot(place, ag[d, :, lo:hi], preferred_element_type=F32)
        send[d * plane:(d + 1) * plane, :, lo:hi] = packed.reshape(plane, CAP, hi - lo).astype(BF16)
        share = jnp.where(table0, facts[2:3, :], 0.0) + jnp.where(table1, facts[3:4, :], 0.0)
        share = share.T
        high = share.astype(BF16)
        high_t[k, d] = high
        low_t[k, d] = (share - high.astype(F32)).astype(BF16)

    def sources(k, group, j):
        return with_dim(k, 0 if group == 0 else others, *j)

    def slot_rows(group, j):
        return (0 if group == 0 else others, *j)

    def dispatch(k, group, j):
        return remote(
            send6.at[(*slot_rows(group, j), slice(None), lanes[k])],
            recv6.at[(*sources(k, group, j), slice(None), lanes[k])],
            out_send.at[group, k], out_recv.at[group, k], dev(with_dim(k, 0, *j)),
        )

    here = (0, 0, 0)

    def keep(k, group):
        return pltpu.make_async_copy(
            send6.at[(*slot_rows(group, here), slice(None), lanes[k])],
            recv6.at[(*sources(k, group, here), slice(None), lanes[k])],
            own_sem.at[group, k],
        )

    def start_group(group):
        for i in range(peers):
            for k in range(3):
                dispatch(k, group, order[(i + k * 10) % peers]).start()
        for k in range(3):
            keep(k, group).start()

    def bulk(buffer, k, blocks, s, r):
        part_of = buffer.at[pl.ds(0, blocks), :, lanes[k]]
        return remote(part_of, part_of, s, r, near)

    for k in range(3):
        pack(k, 0, mine)

    own_up.wait()
    own_down.wait()
    pl.semaphore_wait(barrier, len(greeted))

    def tell(k, d):
        return remote(mine, info.at[k, d], info_send.at[k, d], info_recv.at[k, d], dev(along(k, d)))

    def share_tokens(k, d):
        return remote(
            ag.at[0, :, lanes[k]], ag.at[d, :, lanes[k]], ag_send.at[k, d], ag_recv.at[k, d], dev(along(k, d))
        )

    for d in ring:
        for k in range(3):
            tell(k, d).start()
    for d in ring:
        for k in range(3):
            share_tokens(k, d).start()

    pieces = (
        (0, 0, 384, (0, 1, 2, 3)),
        (0, 384, 512, (1, 2, 0, 3)),
        (1, 0, 256, (1, 2, 0, 3)),
        (1, 256, 512, (2, 0, 1, 3)),
    )

    def piece_copy(p, stage, d, incoming):
        half, lo, hi, turn = pieces[p]
        axis = turn[stage]
        where = list(at)
        for held in turn[:stage]:
            where[held] = slice(None)
        if incoming:
            where[axis] = (at[axis] + dims[axis] - d) % dims[axis]
        block = wide.at[(half, *where, slice(None), pl.ds(lo, hi - lo))]
        offset = along(axis, d)
        return remote(block, block, w_send.at[p, stage, d], w_recv.at[p, stage, d], dev(offset))

    def each(stage, act, incoming=False):
        for p in range(4):
            axis = pieces[p][3][stage]
            for d in range(1, dims[axis]):
                act(piece_copy(p, stage, d, incoming))

    def begin(stage):
        each(stage, lambda copy: copy.start())

    def arrive(stage):
        each(stage, lambda copy: copy.wait_recv(), True)

    def leave(stage):
        each(stage, lambda copy: copy.wait_send())

    begin(0)
    start_group(0)

    for d in ring:
        for k in range(3):
            tell(k, d).wait_recv()
            share_tokens(k, d).wait_recv()
            pack(k, d, info[k, d])
    start_group(1)

    arrive(0)
    begin(1)

    for load in loads:
        load.wait()

    def experts_on(p):
        block = pl.ds(p * plane, plane)
        x_in = recv[block].reshape(plane * CAP, width)
        gate_part = jnp.dot(x_in, v_gate[...], preferred_element_type=F32)
        up_part = jnp.dot(x_in, v_up[...], preferred_element_type=F32)
        hidden = (gate_part / (1.0 + jnp.exp(-gate_part)) * up_part).astype(BF16)
        res = jnp.dot(hidden, v_down[...], preferred_element_type=F32)
        result[block] = res.reshape(plane, CAP, width).astype(BF16)

    for group in range(2):
        for k in range(3):
            keep(k, group).wait()
            blocks = peers * (1 if group == 0 else side - 1)
            bulk(recv, k, blocks, out_send.at[group, k], out_recv.at[group, k]).wait_recv()

    arrive(1)
    begin(2)

    def giveback(k, d, j):
        group = 0 if isinstance(d, int) and d == 0 else 1
        there = minus(with_dim(k, 0, *j))
        src = result6.at[(*with_dim(k, d, *j), slice(None), lanes[k])]
        dst = back6.at[(d, *j, slice(None), lanes[k])]
        if j == here:
            return pltpu.make_async_copy(src, dst, own_sem.at[2, k] if group == 0 else own_sem.at[3, k])
        return remote(src, dst, ret_send.at[group, k], ret_recv.at[group, k], dev(there))

    spread = [here, *order]
    for p in (*ring, 0):
        experts_on(p)
        flat = [j for j in spread if j[0] == p]
        moves = [(1, others, j) for j in flat] + [(2, others, j) for j in flat]
        moves = [m for pair in zip(moves[:len(flat)], moves[len(flat):]) for m in pair]
        if p:
            moves += [(0, p, j) for j in spread if j != here]
        for k, d, j in moves:
            giveback(k, d, j).start()
    for j in order:
        for k in range(3):
            giveback(k, 0, j).start()
    for k in range(3):
        giveback(k, 0, here).start()
    keep_back = pltpu.make_async_copy(
        result6.at[(*with_dim(0, others, *here), slice(None), lanes[0])],
        back6.at[(others, *here, slice(None), lanes[0])], own_sem.at[3, 0],
    )
    keep_back.start()

    arrive(2)
    begin(3)

    def combine(k, d):
        lo, hi = cols[k]
        rows_back = back[d * plane:(d + 1) * plane, :, lo:hi].reshape(slots, hi - lo)
        total = jnp.dot(high_t[k, d], rows_back, preferred_element_type=F32)
        return total + jnp.dot(low_t[k, d], rows_back, preferred_element_type=F32)

    def partial(k, d):
        return remote(
            rs_out.at[d, :, lanes[k]], rs_in.at[d, :, lanes[k]], rs_send.at[k, d], rs_recv.at[k, d],
            dev(along(k, -d % side)),
        )

    keep_back.wait()
    for k in range(3):
        if k:
            giveback(k, others, here).wait()
        bulk(back, k, peers * (side - 1), ret_send.at[1, k], ret_recv.at[1, k]).wait_recv()
        for d in ring:
            lo, hi = cols[k]
            rs_out[d, :, lo:hi] = combine(k, d).astype(BF16)
            partial(k, d).start()

    arrive(3)
    dense_pre = jnp.dot(ag[0], wide[0].reshape(width, -1), preferred_element_type=F32)
    dense_hidden = (dense_pre / (1.0 + jnp.exp(-dense_pre))).astype(BF16)

    for k in range(3):
        lo, hi = cols[k]
        giveback(k, 0, here).wait()
        bulk(back, k, peers, ret_send.at[0, k], ret_recv.at[0, k]).wait_recv()
    dense_out = lax.dot_general(
        dense_hidden, wide[1].reshape(width, -1), (((1,), (1,)), ((), ())), preferred_element_type=F32
    )
    dense_out = jnp.tanh(branch[...]) * dense_out
    for k in range(3):
        lo, hi = cols[k]
        total = combine(k, 0) + dense_out[:, lo:hi]
        for d in ring:
            partial(k, d).wait_recv()
            total = total + rs_in[d, :, lo:hi].astype(F32)
        out[:, lo:hi] = total.astype(BF16)

    for k in range(3):
        for d in ring:
            tell(k, d).wait_send()
            share_tokens(k, d).wait_send()
            partial(k, d).wait_send()
        for group in range(2):
            blocks = peers * (1 if group == 0 else side - 1)
            bulk(send, k, blocks, out_send.at[group, k], out_recv.at[group, k]).wait_send()
            bulk(result, k, blocks, ret_send.at[group, k], ret_recv.at[group, k]).wait_send()
    for stage in range(4):
        leave(stage)


def on_device(tokens, norm_gain, route_ids, route_weight, expert_gate, expert_up, expert_down, dense_up, dense_down, branch_gate):
    n = lax.axis_size("ep")
    assert expert_gate.shape[0] == 1
    rows, width = tokens.shape
    ff = expert_gate.shape[2]
    d_rows, dh = dense_up.shape
    cores = 2
    side = round((n // cores) ** (1 / 3))
    assert side ** 3 * cores == n
    tile = width // 128
    cuts = [tile // 3, tile // 3 * 2, tile]
    cols = tuple((lo * 128, hi * 128) for lo, hi in zip([0, *cuts[:2]], cuts))
    plane = n // side
    vmem = pl.BlockSpec(memory_space=pltpu.VMEM)
    hbm = pl.BlockSpec(memory_space=pl.ANY)
    dma = pltpu.SemaphoreType.DMA
    return pl.pallas_call(
        functools.partial(kernel, side, cores, cols),
        out_shape=jax.ShapeDtypeStruct((rows, width), BF16),
        in_specs=[vmem, vmem, vmem, vmem, hbm, hbm, hbm, hbm, hbm, vmem],
        out_specs=vmem,
        scratch_shapes=[
            pltpu.VMEM((side, rows, width), BF16),
            pltpu.VMEM((8, rows), F32),
            pltpu.VMEM((3, side, 8, rows), F32),
            pltpu.VMEM((n, CAP, width), BF16),
            pltpu.VMEM((n, CAP, width), BF16),
            pltpu.VMEM((n, CAP, width), BF16),
            pltpu.VMEM((n, CAP, width), BF16),
            pltpu.VMEM((side, rows, width), BF16),
            pltpu.VMEM((side, rows, width), BF16),
            pltpu.VMEM((3, side, rows, plane * CAP), BF16),
            pltpu.VMEM((3, side, rows, plane * CAP), BF16),
            pltpu.VMEM((width, ff), BF16),
            pltpu.VMEM((width, ff), BF16),
            pltpu.VMEM((ff, width), BF16),
            pltpu.VMEM((2, side, side, side, cores, d_rows, dh), BF16),
            dma((5,)), dma((3, side)), dma((3, side)), dma((3, side)), dma((3, side)),
            dma((2, 3)), dma((2, 3)), dma((4, 3)),
            dma((2, 3)), dma((2, 3)), dma((3, side)), dma((3, side)),
            dma((4, 4, side)), dma((4, 4, side)),
        ],
        compiler_params=pltpu.CompilerParams(
            collective_id=0, has_side_effects=True, vmem_limit_bytes=62 * 1024 * 1024
        ),
    )(
        tokens, norm_gain.reshape(1, -1), route_ids.T, route_weight.T,
        expert_gate, expert_up, expert_down, dense_up, dense_down.T, branch_gate.reshape(1, -1),
    )


def solution(mesh):
    placed = (
        P("ep", None), P(), P("ep", None), P("ep", None),
        P("ep", None, None), P("ep", None, None), P("ep", None, None),
        P("ep", None), P(None, "ep"), P(),
    )
    return jax.shard_map(
        on_device, mesh=mesh, in_specs=placed, out_specs=P("ep", None), check_vma=False
    )
```

```python
import functools
import itertools
import math

import jax
import jax.numpy as jnp
from jax import lax
from jax.experimental import pallas as pl
from jax.experimental.pallas import tpu as pltpu
from jax.sharding import PartitionSpec as P

CAP = 8
F32 = jnp.float32
BF16 = jnp.bfloat16


def plane_order(side, cores):
    def hop(d):
        return min(d, side - d)

    offsets = [o for o in itertools.product(range(side), range(side), range(cores)) if any(o)]
    order = []
    for o in sorted(offsets, key=lambda o: hop(o[0]) + hop(o[1])):
        for pick in (o, (-o[0] % side, -o[1] % side, o[2])):
            if pick not in order:
                order.append(pick)
    return order


def with_dim(k, d, a, b, e):
    full = [a, b]
    full.insert(k, d)
    return (*full, e)


def kernel(
    side, cores, cols,
    tokens, gain, ids, weight, w_gate, w_up, w_down, d_up, d_down, branch,
    out,
    ag, mine, info, send, recv, result, back, rs_out, rs_in, high_t, low_t, dense, v_gate, v_up, v_down, wide,
    ready, local_sem, info_send, info_recv, ag_send, ag_recv, out_send, out_recv, own_sem,
    ret_send, ret_recv, rs_send, rs_recv, w_send, w_recv,
):
    rows, width = tokens.shape
    plane = side * side * cores
    n = side * plane
    slots = plane * CAP
    me = lax.axis_index("ep")
    dims = (side, side, side, cores)
    strides = (plane, side * cores, cores, 1)
    at = tuple(me // strides[i] % dims[i] for i in range(4))
    part = [[(at[i] + d) % dims[i] * strides[i] for d in range(dims[i])] for i in range(4)]
    grid = (side, side, side, cores, CAP, width)
    by_core = (cores, side, side, side, CAP, width)
    send6, back6 = (r.reshape(*grid) for r in (send, back))
    recv6, result6 = (r.reshape(*by_core) for r in (recv, result))
    ring = sorted(range(1, side), key=lambda d: (min(d, side - d), d))
    others = pl.ds(1, side - 1)
    order = plane_order(side, cores)
    peers = len(order)
    of_core = [[o for o in order if o[2] == e] for e in range(cores)]
    lanes = [pl.ds(lo, hi - lo) for lo, hi in cols]

    def dev(o):
        return part[0][o[0]] + part[1][o[1]] + part[2][o[2]] + part[3][o[3]]

    def minus(o):
        return tuple(-o[i] % dims[i] for i in range(4))

    def along(k, d):
        return tuple(d if i == k else 0 for i in range(4))

    def remote(src, dst, s, r, target):
        return pltpu.make_async_remote_copy(
            src_ref=src, dst_ref=dst, send_sem=s, recv_sem=r,
            device_id=(target,), device_id_type=pl.DeviceIdType.MESH,
        )

    near = dev((0, 0, 0, 1))

    barrier = pltpu.get_barrier_semaphore()
    line = [along(k, d) for d in ring for k in range(3)]
    greeted = line + [(*o[:3], 1) for o in line] + [(0, 0, 0, 1)]

    def greet(semaphore, offsets):
        for o in offsets:
            pl.semaphore_signal(semaphore, inc=1, device_id=(dev(o),), device_id_type=pl.DeviceIdType.MESH)

    greet(barrier, greeted)

    own_up = pltpu.make_async_copy(d_up, wide.at[(0, *at)], local_sem.at[0])
    own_down = pltpu.make_async_copy(d_down, wide.at[(1, *at)], local_sem.at[1])
    own_up.start()
    own_down.start()
    loads = [
        pltpu.make_async_copy(w_gate.at[0], v_gate, local_sem.at[2]),
        pltpu.make_async_copy(w_up.at[0], v_up, local_sem.at[3]),
        pltpu.make_async_copy(w_down.at[0], v_down, local_sem.at[4]),
    ]
    for load in loads:
        load.start()

    x = tokens[...].astype(F32)
    scale = lax.rsqrt(jnp.mean(x * x, axis=-1, keepdims=True) + 1e-06)
    ag[0] = (x * scale * gain[...]).astype(BF16)
    mine[...] = jnp.concatenate(
        [ids[...].astype(F32), weight[...], jnp.zeros((4, rows), F32)], axis=0
    )

    before = lax.broadcasted_iota(jnp.int32, (rows, rows), 0) < lax.broadcasted_iota(jnp.int32, (rows, rows), 1)
    before = before.astype(F32).astype(BF16)
    j_iota = lax.broadcasted_iota(jnp.int32, (plane, rows), 0)
    p_iota = lax.broadcasted_iota(jnp.int32, (slots, rows), 0)

    def slots_of(k, facts):
        first, second = [i for i in range(3) if i != k]

        def local(expert):
            coords = [expert // strides[i] % dims[i] for i in range(4)]
            away = [(coords[i] + dims[i] - at[i]) % dims[i] for i in range(4)]
            j = (away[first] * side + away[second]) * cores + away[3]
            return jnp.where(away[k] == 0, j, -1)

        j0 = local(facts[0:1, :].astype(jnp.int32))
        j1 = local(facts[1:2, :].astype(jnp.int32))
        hot0 = (j0 == j_iota).astype(F32)
        hot1 = (j1 == j_iota).astype(F32)
        count = jnp.dot((hot0 + hot1).astype(BF16), before, preferred_element_type=F32)
        rank0 = jnp.sum(hot0 * count, axis=0, keepdims=True).astype(jnp.int32)
        rank1 = jnp.sum(hot1 * count, axis=0, keepdims=True).astype(jnp.int32)
        slot0 = jnp.where(j0 < 0, -1, j0 * CAP + rank0)
        slot1 = jnp.where(j1 < 0, -1, j1 * CAP + rank1)
        return slot0 == p_iota, slot1 == p_iota

    def pack(k, d, facts):
        lo, hi = cols[k]
        table0, table1 = slots_of(k, facts)
        place = jnp.where(table0 | table1, 1.0, 0.0).astype(BF16)
        packed = jnp.dot(place, ag[d, :, lo:hi], preferred_element_type=F32)
        send[d * plane:(d + 1) * plane, :, lo:hi] = packed.reshape(plane, CAP, hi - lo).astype(BF16)
        share = jnp.where(table0, facts[2:3, :], 0.0) + jnp.where(table1, facts[3:4, :], 0.0)
        share = share.T
        high = share.astype(BF16)
        high_t[k, d] = high
        low_t[k, d] = (share - high.astype(F32)).astype(BF16)

    def core_first(o):
        return (o[3], *o[:3])

    def sources(k, group, j):
        return core_first(with_dim(k, 0 if group == 0 else others, *j))

    def slot_rows(group, j):
        return (0 if group == 0 else others, *j)

    def dispatch(k, group, j):
        return remote(
            send6.at[(*slot_rows(group, j), slice(None), lanes[k])],
            recv6.at[(*sources(k, group, j), slice(None), lanes[k])],
            out_send.at[group + j[2] * (group > 0), k], out_recv.at[group + j[2] * (group > 0), k],
            dev(with_dim(k, 0, *j)),
        )

    here = (0, 0, 0)

    def keep(k, group):
        return pltpu.make_async_copy(
            send6.at[(*slot_rows(group, here), slice(None), lanes[k])],
            recv6.at[(*sources(k, group, here), slice(None), lanes[k])],
            own_sem.at[group, k],
        )

    def start_group(group, targets):
        count = len(targets)
        for i in range(count):
            for k in range(3):
                dispatch(k, group, targets[(i + k * count // 3) % count]).start()

    def bulk(buffer, k, blocks, s, r):
        part_of = buffer.at[pl.ds(0, blocks), :, lanes[k]]
        return remote(part_of, part_of, s, r, near)

    for k in range(3):
        pack(k, 0, mine)

    own_up.wait()
    own_down.wait()
    pl.semaphore_wait(barrier, len(greeted))
    greet(ready, line)

    def tell(k, d):
        return remote(mine, info.at[k, d], info_send.at[k, d], info_recv.at[k, d], dev(along(k, d)))

    def share_tokens(k, d):
        return remote(
            ag.at[0, :, lanes[k]], ag.at[d, :, lanes[k]], ag_send.at[k, d], ag_recv.at[k, d], dev(along(k, d))
        )

    for d in ring:
        for k in range(3):
            tell(k, d).start()
    for d in ring:
        for k in range(3):
            share_tokens(k, d).start()

    pieces = (
        (0, 0, 384, (0, 1, 2, 3)),
        (0, 384, 512, (1, 2, 0, 3)),
        (1, 0, 256, (1, 2, 0, 3)),
        (1, 256, 512, (2, 0, 1, 3)),
    )

    def piece_copy(p, stage, d, incoming):
        half, lo, hi, turn = pieces[p]
        axis = turn[stage]
        where = list(at)
        for held in turn[:stage]:
            where[held] = slice(None)
        if incoming:
            where[axis] = (at[axis] + dims[axis] - d) % dims[axis]
        block = wide.at[(half, *where, slice(None), pl.ds(lo, hi - lo))]
        offset = along(axis, d)
        return remote(block, block, w_send.at[p, stage, d], w_recv.at[p, stage, d], dev(offset))

    def each(stage, act, incoming=False):
        for p in range(4):
            axis = pieces[p][3][stage]
            for d in range(1, dims[axis]):
                act(piece_copy(p, stage, d, incoming))

    def begin(stage):
        each(stage, lambda copy: copy.start())

    def arrive(stage):
        each(stage, lambda copy: copy.wait_recv(), True)

    def leave(stage):
        each(stage, lambda copy: copy.wait_send())

    begin(0)
    pl.semaphore_wait(ready, len(line))
    start_group(0, order)
    for k in range(3):
        keep(k, 0).start()

    for d in ring:
        for k in range(3):
            tell(k, d).wait_recv()
            share_tokens(k, d).wait_recv()
            pack(k, d, info[k, d])
        if d == ring[0]:
            arrive(0)
            begin(1)
    for e in range(cores):
        start_group(1, of_core[e])
    for k in range(3):
        keep(k, 1).start()
    arrive(1)
    begin(2)

    for load in loads:
        load.wait()

    part_rows = n // (2 * cores)

    def experts_on(p):
        block = pl.ds(p * part_rows, part_rows)
        x_in = recv[block].reshape(part_rows * CAP, width)
        gate_part = jnp.dot(x_in, v_gate[...], preferred_element_type=F32)
        up_part = jnp.dot(x_in, v_up[...], preferred_element_type=F32)
        hidden = (gate_part / (1.0 + jnp.exp(-gate_part)) * up_part).astype(BF16)
        res = jnp.dot(hidden, v_down[...], preferred_element_type=F32)
        result[block] = res.reshape(part_rows, CAP, width).astype(BF16)

    def giveback(k, d, j):
        group = 0 if isinstance(d, int) and d == 0 else 1
        there = minus(with_dim(k, 0, *j))
        src = result6.at[(*core_first(with_dim(k, d, *j)), slice(None), lanes[k])]
        dst = back6.at[(d, *j, slice(None), lanes[k])]
        if j == here:
            return pltpu.make_async_copy(src, dst, own_sem.at[2, k] if group == 0 else own_sem.at[3, k])
        return remote(src, dst, ret_send.at[group, k], ret_recv.at[group, k], dev(there))

    def wait_group(group, k, blocks):
        bulk(recv, k, blocks, out_send.at[group, k], out_recv.at[group, k]).wait_recv()

    def start_back(d, targets):
        count = len(targets)
        for i in range(count):
            for k in range(3):
                giveback(k, d, targets[(i + k * count // 3) % count]).start()

    for e in range(cores):
        for k in range(3):
            if e == 0:
                keep(k, 0).wait()
                keep(k, 1).wait()
                wait_group(0, k, peers)
            wait_group(1 + e, k, len(of_core[e]) * (side - 1))
        for p in range(2):
            experts_on(e * 2 + p)
        start_back(others, of_core[e])
    start_back(0, order)
    for k in range(3):
        giveback(k, others, here).start()
        giveback(k, 0, here).start()

    arrive(2)
    begin(3)

    def combine(k, d):
        lo, hi = cols[k]
        rows_back = back[d * plane:(d + 1) * plane, :, lo:hi].reshape(slots, hi - lo)
        total = jnp.dot(high_t[k, d], rows_back, preferred_element_type=F32)
        return total + jnp.dot(low_t[k, d], rows_back, preferred_element_type=F32)

    def partial(k, d):
        return remote(
            rs_out.at[d, :, lanes[k]], rs_in.at[d, :, lanes[k]], rs_send.at[k, d], rs_recv.at[k, d],
            dev(along(k, -d % side)),
        )

    for k in range(3):
        giveback(k, others, here).wait()
        bulk(back, k, peers * (side - 1), ret_send.at[1, k], ret_recv.at[1, k]).wait_recv()
        for d in ring:
            lo, hi = cols[k]
            rs_out[d, :, lo:hi] = combine(k, d).astype(BF16)
            partial(k, d).start()

    arrive(3)
    dense_pre = jnp.dot(ag[0], wide[0].reshape(width, -1), preferred_element_type=F32)
    dense_hidden = (dense_pre / (1.0 + jnp.exp(-dense_pre))).astype(BF16)
    dense_out = lax.dot_general(
        dense_hidden, wide[1].reshape(width, -1), (((1,), (1,)), ((), ())), preferred_element_type=F32
    )
    dense[...] = jnp.tanh(branch[...]) * dense_out
    for k in range(3):
        lo, hi = cols[k]
        giveback(k, 0, here).wait()
        bulk(back, k, peers, ret_send.at[0, k], ret_recv.at[0, k]).wait_recv()
        total = combine(k, 0) + dense[:, lo:hi]
        for d in ring:
            partial(k, d).wait_recv()
            total = total + rs_in[d, :, lo:hi].astype(F32)
        out[:, lo:hi] = total.astype(BF16)

    for k in range(3):
        for d in ring:
            tell(k, d).wait_send()
            share_tokens(k, d).wait_send()
            partial(k, d).wait_send()
        for e in range(cores):
            blocks = len(of_core[e]) * (side - 1)
            bulk(send, k, blocks, out_send.at[1 + e, k], out_recv.at[1 + e, k]).wait_send()
        bulk(send, k, peers, out_send.at[0, k], out_recv.at[0, k]).wait_send()
        for group in range(2):
            blocks = peers * (1 if group == 0 else side - 1)
            bulk(result, k, blocks, ret_send.at[group, k], ret_recv.at[group, k]).wait_send()
    for stage in range(4):
        leave(stage)


def on_device(tokens, norm_gain, route_ids, route_weight, expert_gate, expert_up, expert_down, dense_up, dense_down, branch_gate):
    n = lax.axis_size("ep")
    assert expert_gate.shape[0] == 1
    rows, width = tokens.shape
    ff = expert_gate.shape[2]
    d_rows, dh = dense_up.shape
    cores = 2
    side = round((n // cores) ** (1 / 3))
    assert side ** 3 * cores == n
    tile = width // 128
    cuts = [tile // 3, tile // 3 * 2, tile]
    cols = tuple((lo * 128, hi * 128) for lo, hi in zip([0, *cuts[:2]], cuts))
    plane = n // side
    vmem = pl.BlockSpec(memory_space=pltpu.VMEM)
    hbm = pl.BlockSpec(memory_space=pl.ANY)
    dma = pltpu.SemaphoreType.DMA
    return pl.pallas_call(
        functools.partial(kernel, side, cores, cols),
        out_shape=jax.ShapeDtypeStruct((rows, width), BF16),
        in_specs=[vmem, vmem, vmem, vmem, hbm, hbm, hbm, hbm, hbm, vmem],
        out_specs=vmem,
        scratch_shapes=[
            pltpu.VMEM((side, rows, width), BF16),
            pltpu.VMEM((8, rows), F32),
            pltpu.VMEM((3, side, 8, rows), F32),
            pltpu.VMEM((n, CAP, width), BF16),
            pltpu.VMEM((n, CAP, width), BF16),
            pltpu.VMEM((n, CAP, width), BF16),
            pltpu.VMEM((n, CAP, width), BF16),
            pltpu.VMEM((side, rows, width), BF16),
            pltpu.VMEM((side, rows, width), BF16),
            pltpu.VMEM((3, side, rows, plane * CAP), BF16),
            pltpu.VMEM((3, side, rows, plane * CAP), BF16),
            pltpu.VMEM((rows, width), F32),
            pltpu.VMEM((width, ff), BF16),
            pltpu.VMEM((width, ff), BF16),
            pltpu.VMEM((ff, width), BF16),
            pltpu.VMEM((2, side, side, side, cores, d_rows, dh), BF16),
            pltpu.SemaphoreType.REGULAR,
            dma((5,)), dma((3, side)), dma((3, side)), dma((3, side)), dma((3, side)),
            dma((1 + cores, 3)), dma((1 + cores, 3)), dma((4, 3)),
            dma((2, 3)), dma((2, 3)), dma((3, side)), dma((3, side)),
            dma((4, 4, side)), dma((4, 4, side)),
        ],
        compiler_params=pltpu.CompilerParams(
            collective_id=0, has_side_effects=True, vmem_limit_bytes=62 * 1024 * 1024
        ),
    )(
        tokens, norm_gain.reshape(1, -1), route_ids.T, route_weight.T,
        expert_gate, expert_up, expert_down, dense_up, dense_down.T, branch_gate.reshape(1, -1),
    )


def solution(mesh):
    placed = (
        P("ep", None), P(), P("ep", None), P("ep", None),
        P("ep", None, None), P("ep", None, None), P("ep", None, None),
        P("ep", None), P(None, "ep"), P(),
    )
    return jax.shard_map(
        on_device, mesh=mesh, in_specs=placed, out_specs=P("ep", None), check_vma=False
    )
```

```python
import functools
import itertools
import math

import jax
import jax.numpy as jnp
from jax import lax
from jax.experimental import pallas as pl
from jax.experimental.pallas import tpu as pltpu
from jax.sharding import PartitionSpec as P

CAP = 8
F32 = jnp.float32
BF16 = jnp.bfloat16


def plane_order(side, cores):
    def hop(d):
        return min(d, side - d)

    offsets = [o for o in itertools.product(range(side), range(side), range(cores)) if any(o)]
    order = []
    for o in sorted(offsets, key=lambda o: hop(o[0]) + hop(o[1])):
        for pick in (o, (-o[0] % side, -o[1] % side, o[2])):
            if pick not in order:
                order.append(pick)
    return order


def with_dim(k, d, a, b, e):
    full = [a, b]
    full.insert(k, d)
    return (*full, e)


def kernel(
    side, cores, cols,
    tokens, gain, ids, weight, w_gate, w_up, w_down, d_up, d_down, branch,
    out,
    ag, mine, info, send, recv, result, back, rs_out, rs_in, folded, shares, dense, v_gate, v_up, v_down, wide,
    ready, local_sem, info_send, info_recv, ag_send, ag_recv, out_send, out_recv, own_sem,
    ret_send, ret_recv, rs_send, rs_recv, w_send, w_recv,
    pass_send, pass_recv, fold_send, fold_recv, on_send, on_recv,
):
    rows, width = tokens.shape
    plane = side * side * cores
    n = side * plane
    slots = plane * CAP
    me = lax.axis_index("ep")
    dims = (side, side, side, cores)
    strides = (plane, side * cores, cores, 1)
    at = tuple(me // strides[i] % dims[i] for i in range(4))
    part = [[(at[i] + d) % dims[i] * strides[i] for d in range(dims[i])] for i in range(4)]
    grid = (side, side, side, cores, CAP, width)
    by_core = (cores, side, side, side, CAP, width)
    send6, back6 = (r.reshape(*grid) for r in (send, back))
    recv6, result6 = (r.reshape(*by_core) for r in (recv, result))
    ring = sorted(range(1, side), key=lambda d: (min(d, side - d), d))
    others = pl.ds(1, side - 1)
    order = plane_order(side, cores)
    peers = len(order)
    of_core = [[o for o in order if o[2] == e] for e in range(cores)]
    lanes = [pl.ds(lo, hi - lo) for lo, hi in cols]

    def dev(o):
        return part[0][o[0]] + part[1][o[1]] + part[2][o[2]] + part[3][o[3]]

    def minus(o):
        return tuple(-o[i] % dims[i] for i in range(4))

    def along(k, d):
        return tuple(d if i == k else 0 for i in range(4))

    def remote(src, dst, s, r, target):
        return pltpu.make_async_remote_copy(
            src_ref=src, dst_ref=dst, send_sem=s, recv_sem=r,
            device_id=(target,), device_id_type=pl.DeviceIdType.MESH,
        )

    near = dev((0, 0, 0, 1))

    barrier = pltpu.get_barrier_semaphore()
    line = [along(k, d) for d in ring for k in range(3)]
    greeted = line + [(*o[:3], 1) for o in line] + [(0, 0, 0, 1)]

    def greet(semaphore, offsets):
        for o in offsets:
            pl.semaphore_signal(semaphore, inc=1, device_id=(dev(o),), device_id_type=pl.DeviceIdType.MESH)

    greet(barrier, greeted)

    own_up = pltpu.make_async_copy(d_up, wide.at[(0, *at)], local_sem.at[0])
    own_down = pltpu.make_async_copy(d_down, wide.at[(1, *at)], local_sem.at[1])
    own_up.start()
    own_down.start()
    loads = [
        pltpu.make_async_copy(w_gate.at[0], v_gate, local_sem.at[2]),
        pltpu.make_async_copy(w_up.at[0], v_up, local_sem.at[3]),
        pltpu.make_async_copy(w_down.at[0], v_down, local_sem.at[4]),
    ]
    for load in loads:
        load.start()

    x = tokens[...].astype(F32)
    scale = lax.rsqrt(jnp.mean(x * x, axis=-1, keepdims=True) + 1e-06)
    ag[0] = (x * scale * gain[...]).astype(BF16)
    mine[...] = jnp.concatenate(
        [ids[...].astype(F32), weight[...], jnp.zeros((4, rows), F32)], axis=0
    )

    before = lax.broadcasted_iota(jnp.int32, (rows, rows), 0) < lax.broadcasted_iota(jnp.int32, (rows, rows), 1)
    before = before.astype(F32).astype(BF16)
    j_iota = lax.broadcasted_iota(jnp.int32, (plane, rows), 0)
    p_iota = lax.broadcasted_iota(jnp.int32, (slots, rows), 0)

    def slots_of(k, facts):
        first, second = [i for i in range(3) if i != k]

        def local(expert):
            coords = [expert // strides[i] % dims[i] for i in range(4)]
            away = [(coords[i] + dims[i] - at[i]) % dims[i] for i in range(4)]
            j = (away[first] * side + away[second]) * cores + away[3]
            return jnp.where(away[k] == 0, j, -1)

        j0 = local(facts[0:1, :].astype(jnp.int32))
        j1 = local(facts[1:2, :].astype(jnp.int32))
        hot0 = (j0 == j_iota).astype(F32)
        hot1 = (j1 == j_iota).astype(F32)
        count = jnp.dot((hot0 + hot1).astype(BF16), before, preferred_element_type=F32)
        rank0 = jnp.sum(hot0 * count, axis=0, keepdims=True).astype(jnp.int32)
        rank1 = jnp.sum(hot1 * count, axis=0, keepdims=True).astype(jnp.int32)
        slot0 = jnp.where(j0 < 0, -1, j0 * CAP + rank0)
        slot1 = jnp.where(j1 < 0, -1, j1 * CAP + rank1)
        return slot0 == p_iota, slot1 == p_iota

    def pack(k, d, facts):
        lo, hi = cols[k]
        table0, table1 = slots_of(k, facts)
        place = jnp.where(table0 | table1, 1.0, 0.0).astype(BF16)
        packed = jnp.dot(place, ag[d, :, lo:hi], preferred_element_type=F32)
        send[d * plane:(d + 1) * plane, :, lo:hi] = packed.reshape(plane, CAP, hi - lo).astype(BF16)
        share = jnp.where(table0, facts[2:3, :], 0.0) + jnp.where(table1, facts[3:4, :], 0.0)
        share = share.T
        high = share.astype(BF16)
        shares[k, d, :rows] = high
        shares[k, d, rows:] = (share - high.astype(F32)).astype(BF16)

    def core_first(o):
        return (o[3], *o[:3])

    def sources(k, group, j):
        return core_first(with_dim(k, 0 if group == 0 else others, *j))

    def slot_rows(group, j):
        return (0 if group == 0 else others, *j)

    def dispatch(k, group, d, j):
        return remote(
            send6.at[(d, *j, slice(None), lanes[k])],
            recv6.at[(*core_first(with_dim(k, d, *j)), slice(None), lanes[k])],
            out_send.at[group, k], out_recv.at[group, k], dev(with_dim(k, 0, *j)),
        )

    here = (0, 0, 0)

    def keep(k, group):
        return pltpu.make_async_copy(
            send6.at[(*slot_rows(group, here), slice(None), lanes[k])],
            recv6.at[(*sources(k, group, here), slice(None), lanes[k])],
            own_sem.at[group, k],
        )

    def turns(targets):
        count = len(targets)
        return [(k, targets[(i + k * count // 3) % count]) for i in range(count) for k in range(3)]

    def start_own(e):
        for k, j in turns(of_core[e]):
            dispatch(k, 0, 0, j).start()

    def start_ring(e):
        def round_of(d, carry):
            for k, j in turns(of_core[e]):
                dispatch(k, 1 + e, d, j).start()
            return carry

        lax.fori_loop(1, side, round_of, 0)

    def bulk(buffer, k, blocks, s, r):
        part_of = buffer.at[pl.ds(0, blocks), :, lanes[k]]
        return remote(part_of, part_of, s, r, near)

    for k in range(3):
        pack(k, 0, mine)

    own_up.wait()
    own_down.wait()
    pl.semaphore_wait(barrier, len(greeted))
    greet(ready, line)

    def tell(k, d):
        return remote(mine, info.at[k, d], info_send.at[k, d], info_recv.at[k, d], dev(along(k, d)))

    def share_tokens(k, d):
        return remote(
            ag.at[0, :, lanes[k]], ag.at[d, :, lanes[k]], ag_send.at[k, d], ag_recv.at[k, d], dev(along(k, d))
        )

    for d in ring:
        for k in range(3):
            tell(k, d).start()
    half = rows // 2
    beside = (1, side - 1)

    def pass_on(k, i):
        d = beside[i]
        part_of = pl.ds(i * half, half)
        return remote(
            ag.at[d, part_of, lanes[k]], ag.at[2, part_of, lanes[k]],
            pass_send.at[k, i], pass_recv.at[k, i], dev(along(k, d)),
        )

    for d in beside:
        for k in range(3):
            share_tokens(k, d).start()

    pieces = (
        (0, 0, 384, (0, 1, 2, 3)),
        (0, 384, 512, (1, 2, 0, 3)),
        (1, 0, 256, (1, 2, 0, 3)),
        (1, 256, 512, (2, 0, 1, 3)),
    )

    def piece_copy(p, stage, d, incoming):
        which, lo, hi, turn = pieces[p]
        axis = turn[stage]
        where = list(at)
        for held in turn[:stage]:
            where[held] = slice(None)
        if incoming:
            where[axis] = (at[axis] + dims[axis] - d) % dims[axis]
        block = wide.at[(which, *where, slice(None), pl.ds(lo, hi - lo))]
        offset = along(axis, d)
        return remote(block, block, w_send.at[p, stage, d], w_recv.at[p, stage, d], dev(offset))

    def each(stage, act, incoming=False):
        for p in range(4):
            axis = pieces[p][3][stage]
            for d in beside if stage == 2 else range(1, dims[axis]):
                act(piece_copy(p, stage, d, incoming))

    def piece_on(p, i, incoming):
        which, lo, hi, turn = pieces[p]
        axis = turn[2]
        where = list(at)
        where[turn[0]] = pl.ds(i * (side // 2), side // 2)
        where[turn[1]] = slice(None)
        where[axis] = (at[axis] + side - (2 if incoming else beside[i])) % side
        block = wide.at[(which, *where, slice(None), pl.ds(lo, hi - lo))]
        return remote(block, block, on_send.at[p, i], on_recv.at[p, i], dev(along(axis, beside[i])))

    def begin(stage):
        each(stage, lambda copy: copy.start())

    def arrive(stage):
        each(stage, lambda copy: copy.wait_recv(), True)

    def leave(stage):
        each(stage, lambda copy: copy.wait_send())

    begin(0)
    pl.semaphore_wait(ready, len(line))
    start_own(0)

    for i in range(2):
        for k in range(3):
            share_tokens(k, beside[i]).wait_recv()
            pass_on(k, i).start()
    start_own(1)
    for d in beside:
        for k in range(3):
            tell(k, d).wait_recv()
            pack(k, d, info[k, d])
    arrive(0)
    begin(1)
    for k in range(3):
        keep(k, 0).start()
        tell(k, 2).wait_recv()
        for i in range(2):
            pass_on(k, i).wait_recv()
        pack(k, 2, info[k, 2])
    for e in range(cores):
        start_ring(e)
    for k in range(3):
        keep(k, 1).start()
    arrive(1)
    begin(2)

    for load in loads:
        load.wait()

    part_rows = n // (2 * cores)

    def experts_on(p):
        block = pl.ds(p * part_rows, part_rows)
        x_in = recv[block].reshape(part_rows * CAP, width)
        gate_part = jnp.dot(x_in, v_gate[...], preferred_element_type=F32)
        up_part = jnp.dot(x_in, v_up[...], preferred_element_type=F32)
        hidden = (gate_part / (1.0 + jnp.exp(-gate_part)) * up_part).astype(BF16)
        res = jnp.dot(hidden, v_down[...], preferred_element_type=F32)
        result[block] = res.reshape(part_rows, CAP, width).astype(BF16)

    def giveback(k, group, d, j):
        return remote(
            result6.at[(*core_first(with_dim(k, d, *j)), slice(None), lanes[k])],
            back6.at[(d, *j, slice(None), lanes[k])],
            ret_send.at[group, k], ret_recv.at[group, k], dev(minus(with_dim(k, 0, *j))),
        )

    def keep_back(k, group):
        d = others if group else 0
        return pltpu.make_async_copy(
            result6.at[(*core_first(with_dim(k, d, *here)), slice(None), lanes[k])],
            back6.at[(d, *here, slice(None), lanes[k])], own_sem.at[2 + group, k],
        )

    def wait_group(group, k, blocks):
        bulk(recv, k, blocks, out_send.at[group, k], out_recv.at[group, k]).wait_recv()

    def back_own(e):
        for k, j in turns(of_core[e]):
            giveback(k, 0, 0, j).start()

    def back_ring(e):
        def round_of(d, carry):
            for k, j in turns(of_core[e]):
                giveback(k, 1, d, j).start()
            return carry

        lax.fori_loop(1, side, round_of, 0)

    for e in range(cores):
        for k in range(3):
            if e == 0:
                keep(k, 0).wait()
                keep(k, 1).wait()
                wait_group(0, k, peers)
            wait_group(1 + e, k, len(of_core[e]) * (side - 1))
        for p in range(2):
            experts_on(e * 2 + p)
        back_ring(e)
    arrive(2)
    for p in range(4):
        for i in range(2):
            piece_on(p, i, False).start()
    back_own(0)
    for k in range(3):
        keep_back(k, 1).start()
        keep_back(k, 0).start()

    def combine(k, d):
        lo, hi = cols[k]
        rows_back = back[d * plane:(d + 1) * plane, :, lo:hi].reshape(slots, hi - lo)
        total = jnp.dot(shares[k, d], rows_back, preferred_element_type=F32)
        return total[:rows] + total[rows:]

    def partial(k, d):
        return remote(
            rs_out.at[d, :, lanes[k]], rs_in.at[d, :, lanes[k]], rs_send.at[k, d], rs_recv.at[k, d],
            dev(along(k, -d % side)),
        )

    def fold(k, i):
        part_of = pl.ds(i * half, half)
        return remote(
            rs_out.at[2, part_of, lanes[k]], folded.at[i, :, lanes[k]],
            fold_send.at[k, i], fold_recv.at[k, i], dev(along(k, -beside[i] % side)),
        )

    for k in range(3):
        lo, hi = cols[k]
        keep_back(k, 1).wait()
        bulk(back, k, peers * (side - 1), ret_send.at[1, k], ret_recv.at[1, k]).wait_recv()
        rs_out[2, :, lo:hi] = combine(k, 2).astype(BF16)
        for i in range(2):
            fold(k, i).start()
    back_own(1)
    for p in range(4):
        for i in range(2):
            piece_on(p, i, True).wait_recv()
    begin(3)
    for k in range(3):
        lo, hi = cols[k]
        for i in range(2):
            total = combine(k, beside[i])
            fold(k, i).wait_recv()
            mixed = total[i * half:(i + 1) * half] + folded[i, :, lo:hi].astype(F32)
            rest = total[(1 - i) * half:(2 - i) * half]
            rs_out[beside[i], i * half:(i + 1) * half, lo:hi] = mixed.astype(BF16)
            rs_out[beside[i], (1 - i) * half:(2 - i) * half, lo:hi] = rest.astype(BF16)
            partial(k, beside[i]).start()

    arrive(3)
    dense_pre = jnp.dot(ag[0], wide[0].reshape(width, -1), preferred_element_type=F32)
    dense_hidden = (dense_pre / (1.0 + jnp.exp(-dense_pre))).astype(BF16)
    dense_out = lax.dot_general(
        dense_hidden, wide[1].reshape(width, -1), (((1,), (1,)), ((), ())), preferred_element_type=F32
    )
    dense[...] = jnp.tanh(branch[...]) * dense_out
    for k in range(3):
        lo, hi = cols[k]
        keep_back(k, 0).wait()
        bulk(back, k, peers, ret_send.at[0, k], ret_recv.at[0, k]).wait_recv()
        total = combine(k, 0) + dense[:, lo:hi]
        for d in beside:
            partial(k, d).wait_recv()
            total = total + rs_in[d, :, lo:hi].astype(F32)
        out[:, lo:hi] = total.astype(BF16)

    for k in range(3):
        for d in ring:
            tell(k, d).wait_send()
        for i in range(2):
            share_tokens(k, beside[i]).wait_send()
            pass_on(k, i).wait_send()
            fold(k, i).wait_send()
            partial(k, beside[i]).wait_send()
        for e in range(cores):
            blocks = len(of_core[e]) * (side - 1)
            bulk(send, k, blocks, out_send.at[1 + e, k], out_recv.at[1 + e, k]).wait_send()
        bulk(send, k, peers, out_send.at[0, k], out_recv.at[0, k]).wait_send()
        for group in range(2):
            blocks = peers * (1 if group == 0 else side - 1)
            bulk(result, k, blocks, ret_send.at[group, k], ret_recv.at[group, k]).wait_send()
    for stage in range(4):
        leave(stage)
    for p in range(4):
        for i in range(2):
            piece_on(p, i, False).wait_send()


def on_device(tokens, norm_gain, route_ids, route_weight, expert_gate, expert_up, expert_down, dense_up, dense_down, branch_gate):
    n = lax.axis_size("ep")
    assert expert_gate.shape[0] == 1
    rows, width = tokens.shape
    ff = expert_gate.shape[2]
    d_rows, dh = dense_up.shape
    cores = 2
    side = round((n // cores) ** (1 / 3))
    assert side == 4 and side ** 3 * cores == n
    tile = width // 128
    cuts = [tile // 3, tile // 3 * 2, tile]
    cols = tuple((lo * 128, hi * 128) for lo, hi in zip([0, *cuts[:2]], cuts))
    plane = n // side
    vmem = pl.BlockSpec(memory_space=pltpu.VMEM)
    hbm = pl.BlockSpec(memory_space=pl.ANY)
    dma = pltpu.SemaphoreType.DMA
    return pl.pallas_call(
        functools.partial(kernel, side, cores, cols),
        out_shape=jax.ShapeDtypeStruct((rows, width), BF16),
        in_specs=[vmem, vmem, vmem, vmem, hbm, hbm, hbm, hbm, hbm, vmem],
        out_specs=vmem,
        scratch_shapes=[
            pltpu.VMEM((side, rows, width), BF16),
            pltpu.VMEM((8, rows), F32),
            pltpu.VMEM((3, side, 8, rows), F32),
            pltpu.VMEM((n, CAP, width), BF16),
            pltpu.VMEM((n, CAP, width), BF16),
            pltpu.VMEM((n, CAP, width), BF16),
            pltpu.VMEM((n, CAP, width), BF16),
            pltpu.VMEM((side, rows, width), BF16),
            pltpu.VMEM((side, rows, width), BF16),
            pltpu.VMEM((2, rows // 2, width), BF16),
            pltpu.VMEM((3, side, 2 * rows, plane * CAP), BF16),
            pltpu.VMEM((rows, width), F32),
            pltpu.VMEM((width, ff), BF16),
            pltpu.VMEM((width, ff), BF16),
            pltpu.VMEM((ff, width), BF16),
            pltpu.VMEM((2, side, side, side, cores, d_rows, dh), BF16),
            pltpu.SemaphoreType.REGULAR,
            dma((5,)), dma((3, side)), dma((3, side)), dma((3, side)), dma((3, side)),
            dma((1 + cores, 3)), dma((1 + cores, 3)), dma((4, 3)),
            dma((2, 3)), dma((2, 3)), dma((3, side)), dma((3, side)),
            dma((4, 4, side)), dma((4, 4, side)),
            dma((3, 2)), dma((3, 2)), dma((3, 2)), dma((3, 2)), dma((4, 2)), dma((4, 2)),
        ],
        compiler_params=pltpu.CompilerParams(
            collective_id=0, has_side_effects=True, vmem_limit_bytes=62 * 1024 * 1024
        ),
    )(
        tokens, norm_gain.reshape(1, -1), route_ids.T, route_weight.T,
        expert_gate, expert_up, expert_down, dense_up, dense_down.T, branch_gate.reshape(1, -1),
    )


def solution(mesh):
    placed = (
        P("ep", None), P(), P("ep", None), P("ep", None),
        P("ep", None, None), P("ep", None, None), P("ep", None, None),
        P("ep", None), P(None, "ep"), P(),
    )
    return jax.shard_map(
        on_device, mesh=mesh, in_specs=placed, out_specs=P("ep", None), check_vma=False
    )
```

```python
import functools
import itertools
import math

import jax
import jax.numpy as jnp
from jax import lax
from jax.experimental import pallas as pl
from jax.experimental.pallas import tpu as pltpu
from jax.sharding import PartitionSpec as P

CAP = 8
F32 = jnp.float32
BF16 = jnp.bfloat16


def plane_order(side, cores):
    def hop(d):
        return min(d, side - d)

    offsets = [o for o in itertools.product(range(side), range(side), range(cores)) if any(o)]
    order = []
    for o in sorted(offsets, key=lambda o: hop(o[0]) + hop(o[1])):
        for pick in (o, (-o[0] % side, -o[1] % side, o[2])):
            if pick not in order:
                order.append(pick)
    return order


def with_dim(k, d, a, b, e):
    full = [a, b]
    full.insert(k, d)
    return (*full, e)


def kernel(
    side, cores, cols,
    tokens, gain, ids, weight, w_gate, w_up, w_down, d_up, d_down, branch,
    out,
    ag, mine, info, send, recv, result, back, rs_out, rs_in, folded, shares, dense, mixed_rows, v_gate, v_up, v_down, wide,
    ready, local_sem, info_send, info_recv, ag_send, ag_recv, out_send, out_recv, own_sem,
    ret_send, ret_recv, rs_send, rs_recv, w_send, w_recv,
    pass_send, pass_recv, fold_send, fold_recv, on_send, on_recv, emit_sem,
):
    rows, width = tokens.shape
    plane = side * side * cores
    n = side * plane
    slots = plane * CAP
    me = lax.axis_index("ep")
    dims = (side, side, side, cores)
    strides = (plane, side * cores, cores, 1)
    at = tuple(me // strides[i] % dims[i] for i in range(4))
    part = [[(at[i] + d) % dims[i] * strides[i] for d in range(dims[i])] for i in range(4)]
    grid = (side, side, side, cores, CAP, width)
    by_core = (cores, side, side, side, CAP, width)
    send6, back6 = (r.reshape(*grid) for r in (send, back))
    recv6, result6 = (r.reshape(*by_core) for r in (recv, result))
    ring = sorted(range(1, side), key=lambda d: (min(d, side - d), d))
    others = pl.ds(1, side - 1)
    order = plane_order(side, cores)
    peers = len(order)
    of_core = [[o for o in order if o[2] == e] for e in range(cores)]
    lanes = [pl.ds(lo, hi - lo) for lo, hi in cols]

    def dev(o):
        return part[0][o[0]] + part[1][o[1]] + part[2][o[2]] + part[3][o[3]]

    def minus(o):
        return tuple(-o[i] % dims[i] for i in range(4))

    def along(k, d):
        return tuple(d if i == k else 0 for i in range(4))

    def remote(src, dst, s, r, target):
        return pltpu.make_async_remote_copy(
            src_ref=src, dst_ref=dst, send_sem=s, recv_sem=r,
            device_id=(target,), device_id_type=pl.DeviceIdType.MESH,
        )

    near = dev((0, 0, 0, 1))

    barrier = pltpu.get_barrier_semaphore()
    line = [along(k, d) for d in ring for k in range(3)]
    greeted = line + [(*o[:3], 1) for o in line] + [(0, 0, 0, 1)]

    def greet(semaphore, offsets):
        for o in offsets:
            pl.semaphore_signal(semaphore, inc=1, device_id=(dev(o),), device_id_type=pl.DeviceIdType.MESH)

    greet(barrier, greeted)

    own_up = pltpu.make_async_copy(d_up, wide.at[(0, *at)], local_sem.at[0])
    own_down = pltpu.make_async_copy(d_down, wide.at[(1, *at)], local_sem.at[1])
    own_up.start()
    own_down.start()
    loads = [
        pltpu.make_async_copy(w_gate.at[0], v_gate, local_sem.at[2]),
        pltpu.make_async_copy(w_up.at[0], v_up, local_sem.at[3]),
        pltpu.make_async_copy(w_down.at[0], v_down, local_sem.at[4]),
    ]
    for load in loads:
        load.start()

    x = tokens[...].astype(F32)
    scale = lax.rsqrt(jnp.mean(x * x, axis=-1, keepdims=True) + 1e-06)
    ag[0] = (x * scale * gain[...]).astype(BF16)
    mine[...] = jnp.concatenate(
        [ids[...].astype(F32), weight[...], jnp.zeros((4, rows), F32)], axis=0
    )

    before = lax.broadcasted_iota(jnp.int32, (rows, rows), 0) < lax.broadcasted_iota(jnp.int32, (rows, rows), 1)
    before = before.astype(F32).astype(BF16)
    j_iota = lax.broadcasted_iota(jnp.int32, (plane, rows), 0)
    p_iota = lax.broadcasted_iota(jnp.int32, (slots, rows), 0)

    def slots_of(k, facts):
        first, second = [i for i in range(3) if i != k]

        def local(expert):
            coords = [expert // strides[i] % dims[i] for i in range(4)]
            away = [(coords[i] + dims[i] - at[i]) % dims[i] for i in range(4)]
            j = (away[first] * side + away[second]) * cores + away[3]
            return jnp.where(away[k] == 0, j, -1)

        j0 = local(facts[0:1, :].astype(jnp.int32))
        j1 = local(facts[1:2, :].astype(jnp.int32))
        hot0 = (j0 == j_iota).astype(F32)
        hot1 = (j1 == j_iota).astype(F32)
        count = jnp.dot((hot0 + hot1).astype(BF16), before, preferred_element_type=F32)
        rank0 = jnp.sum(hot0 * count, axis=0, keepdims=True).astype(jnp.int32)
        rank1 = jnp.sum(hot1 * count, axis=0, keepdims=True).astype(jnp.int32)
        slot0 = jnp.where(j0 < 0, -1, j0 * CAP + rank0)
        slot1 = jnp.where(j1 < 0, -1, j1 * CAP + rank1)
        return slot0 == p_iota, slot1 == p_iota

    def pack(k, d, facts):
        lo, hi = cols[k]
        table0, table1 = slots_of(k, facts)
        place = jnp.where(table0 | table1, 1.0, 0.0).astype(BF16)
        packed = jnp.dot(place, ag[d, :, lo:hi], preferred_element_type=F32)
        send[d * plane:(d + 1) * plane, :, lo:hi] = packed.reshape(plane, CAP, hi - lo).astype(BF16)
        share = jnp.where(table0, facts[2:3, :], 0.0) + jnp.where(table1, facts[3:4, :], 0.0)
        share = share.T
        high = share.astype(BF16)
        shares[k, d, :rows] = high
        shares[k, d, rows:] = (share - high.astype(F32)).astype(BF16)

    def core_first(o):
        return (o[3], *o[:3])

    def sources(k, group, j):
        return core_first(with_dim(k, 0 if group == 0 else others, *j))

    def slot_rows(group, j):
        return (0 if group == 0 else others, *j)

    def dispatch(k, group, d, j):
        return remote(
            send6.at[(d, *j, slice(None), lanes[k])],
            recv6.at[(*core_first(with_dim(k, d, *j)), slice(None), lanes[k])],
            out_send.at[group, k], out_recv.at[group, k], dev(with_dim(k, 0, *j)),
        )

    here = (0, 0, 0)

    def keep(k, group):
        return pltpu.make_async_copy(
            send6.at[(*slot_rows(group, here), slice(None), lanes[k])],
            recv6.at[(*sources(k, group, here), slice(None), lanes[k])],
            own_sem.at[group, k],
        )

    def turns(targets):
        count = len(targets)
        return [(k, targets[(i + k * count // 3) % count]) for i in range(count) for k in range(3)]

    def start_own(e):
        for k, j in turns(of_core[e]):
            dispatch(k, 0, 0, j).start()

    def start_ring(e):
        def round_of(d, carry):
            for k, j in turns(of_core[e]):
                dispatch(k, 1 + e, d, j).start()
            return carry

        lax.fori_loop(1, side, round_of, 0)

    def bulk(buffer, k, blocks, s, r):
        part_of = buffer.at[pl.ds(0, blocks), :, lanes[k]]
        return remote(part_of, part_of, s, r, near)

    for k in range(3):
        pack(k, 0, mine)

    own_up.wait()
    own_down.wait()
    pl.semaphore_wait(barrier, len(greeted))
    greet(ready, line)

    def tell(k, d):
        return remote(mine, info.at[k, d], info_send.at[k, d], info_recv.at[k, d], dev(along(k, d)))

    def share_tokens(k, d):
        return remote(
            ag.at[0, :, lanes[k]], ag.at[d, :, lanes[k]], ag_send.at[k, d], ag_recv.at[k, d], dev(along(k, d))
        )

    for d in ring:
        for k in range(3):
            tell(k, d).start()
    half = rows // 2
    beside = (1, side - 1)

    def pass_on(k, i):
        d = beside[i]
        part_of = pl.ds(i * half, half)
        return remote(
            ag.at[d, part_of, lanes[k]], ag.at[2, part_of, lanes[k]],
            pass_send.at[k, i], pass_recv.at[k, i], dev(along(k, d)),
        )

    for d in beside:
        for k in range(3):
            share_tokens(k, d).start()

    pieces = (
        (0, 0, 256, (0, 1, 2, 3)),
        (0, 256, 512, (1, 0, 2, 3)),
        (1, 0, 256, (1, 2, 0, 3)),
        (1, 256, 512, (2, 0, 1, 3)),
    )

    def piece_copy(p, stage, d, incoming):
        which, lo, hi, turn = pieces[p]
        axis = turn[stage]
        where = list(at)
        for held in turn[:stage]:
            where[held] = slice(None)
        if incoming:
            where[axis] = (at[axis] + dims[axis] - d) % dims[axis]
        block = wide.at[(which, *where, slice(None), pl.ds(lo, hi - lo))]
        offset = along(axis, d)
        return remote(block, block, w_send.at[p, stage, d], w_recv.at[p, stage, d], dev(offset))

    def each(stage, act, incoming=False):
        for p in range(4):
            axis = pieces[p][3][stage]
            for d in beside if stage == 2 else range(1, dims[axis]):
                act(piece_copy(p, stage, d, incoming))

    def piece_on(p, i, incoming):
        which, lo, hi, turn = pieces[p]
        axis = turn[2]
        where = list(at)
        where[turn[0]] = pl.ds(i * (side // 2), side // 2)
        where[turn[1]] = slice(None)
        where[axis] = (at[axis] + side - (2 if incoming else beside[i])) % side
        block = wide.at[(which, *where, slice(None), pl.ds(lo, hi - lo))]
        return remote(block, block, on_send.at[p, i], on_recv.at[p, i], dev(along(axis, beside[i])))

    def begin(stage):
        each(stage, lambda copy: copy.start())

    def arrive(stage):
        each(stage, lambda copy: copy.wait_recv(), True)

    def leave(stage):
        each(stage, lambda copy: copy.wait_send())

    begin(0)
    pl.semaphore_wait(ready, len(line))
    start_own(0)

    for i in range(2):
        for k in range(3):
            share_tokens(k, beside[i]).wait_recv()
            pass_on(k, i).start()
    start_own(1)
    for d in beside:
        for k in range(3):
            tell(k, d).wait_recv()
            pack(k, d, info[k, d])
    arrive(0)
    begin(1)
    for k in range(3):
        keep(k, 0).start()
        tell(k, 2).wait_recv()
        for i in range(2):
            pass_on(k, i).wait_recv()
        pack(k, 2, info[k, 2])
    for e in range(cores):
        start_ring(e)
    for k in range(3):
        keep(k, 1).start()
    arrive(1)
    begin(2)

    for load in loads:
        load.wait()

    part_rows = n // (2 * cores)

    def experts_on(p):
        block = pl.ds(p * part_rows, part_rows)
        x_in = recv[block].reshape(part_rows * CAP, width)
        gate_part = jnp.dot(x_in, v_gate[...], preferred_element_type=F32)
        up_part = jnp.dot(x_in, v_up[...], preferred_element_type=F32)
        hidden = (gate_part / (1.0 + jnp.exp(-gate_part)) * up_part).astype(BF16)
        res = jnp.dot(hidden, v_down[...], preferred_element_type=F32)
        result[block] = res.reshape(part_rows, CAP, width).astype(BF16)

    def giveback(k, group, d, j):
        return remote(
            result6.at[(*core_first(with_dim(k, d, *j)), slice(None), lanes[k])],
            back6.at[(d, *j, slice(None), lanes[k])],
            ret_send.at[group, k], ret_recv.at[group, k], dev(minus(with_dim(k, 0, *j))),
        )

    def keep_back(k, group):
        d = others if group else 0
        return pltpu.make_async_copy(
            result6.at[(*core_first(with_dim(k, d, *here)), slice(None), lanes[k])],
            back6.at[(d, *here, slice(None), lanes[k])], own_sem.at[2 + group, k],
        )

    def wait_group(group, k, blocks):
        bulk(recv, k, blocks, out_send.at[group, k], out_recv.at[group, k]).wait_recv()

    def back_own(e):
        for k, j in turns(of_core[e]):
            giveback(k, 0, 0, j).start()

    def back_ring(e):
        def round_of(d, carry):
            for k, j in turns(of_core[e]):
                giveback(k, 1, d, j).start()
            return carry

        lax.fori_loop(1, side, round_of, 0)

    for e in range(cores):
        for k in range(3):
            if e == 0:
                keep(k, 0).wait()
                keep(k, 1).wait()
                wait_group(0, k, peers)
            wait_group(1 + e, k, len(of_core[e]) * (side - 1))
        for p in range(2):
            experts_on(e * 2 + p)
        back_ring(e)
    arrive(2)
    for p in range(4):
        for i in range(2):
            piece_on(p, i, False).start()
    back_own(0)
    for k in range(3):
        keep_back(k, 1).start()
        keep_back(k, 0).start()

    def combine(k, d):
        lo, hi = cols[k]
        rows_back = back[d * plane:(d + 1) * plane, :, lo:hi].reshape(slots, hi - lo)
        total = jnp.dot(shares[k, d], rows_back, preferred_element_type=F32)
        return total[:rows] + total[rows:]

    def partial(k, d):
        return remote(
            rs_out.at[d, :, lanes[k]], rs_in.at[d, :, lanes[k]], rs_send.at[k, d], rs_recv.at[k, d],
            dev(along(k, -d % side)),
        )

    def fold(k, i):
        part_of = pl.ds(i * half, half)
        return remote(
            rs_out.at[2, part_of, lanes[k]], folded.at[i, :, lanes[k]],
            fold_send.at[k, i], fold_recv.at[k, i], dev(along(k, -beside[i] % side)),
        )

    for k in range(3):
        lo, hi = cols[k]
        keep_back(k, 1).wait()
        bulk(back, k, peers * (side - 1), ret_send.at[1, k], ret_recv.at[1, k]).wait_recv()
        rs_out[2, :, lo:hi] = combine(k, 2).astype(BF16)
        for i in range(2):
            fold(k, i).start()
    back_own(1)
    for p in range(4):
        for i in range(2):
            piece_on(p, i, True).wait_recv()
    begin(3)
    for k in range(3):
        lo, hi = cols[k]
        for i in range(2):
            total = combine(k, beside[i])
            fold(k, i).wait_recv()
            mixed = total[i * half:(i + 1) * half] + folded[i, :, lo:hi].astype(F32)
            rest = total[(1 - i) * half:(2 - i) * half]
            rs_out[beside[i], i * half:(i + 1) * half, lo:hi] = mixed.astype(BF16)
            rs_out[beside[i], (1 - i) * half:(2 - i) * half, lo:hi] = rest.astype(BF16)
            partial(k, beside[i]).start()

    arrive(3)
    dense_pre = jnp.dot(ag[0], wide[0].reshape(width, -1), preferred_element_type=F32)
    dense_hidden = (dense_pre / (1.0 + jnp.exp(-dense_pre))).astype(BF16)
    dense_out = lax.dot_general(
        dense_hidden, wide[1].reshape(width, -1), (((1,), (1,)), ((), ())), preferred_element_type=F32
    )
    dense[...] = jnp.tanh(branch[...]) * dense_out
    for k in range(3):
        lo, hi = cols[k]
        keep_back(k, 0).wait()
        bulk(back, k, peers, ret_send.at[0, k], ret_recv.at[0, k]).wait_recv()
        dense[:, lo:hi] += combine(k, 0)

    def emit(k):
        return pltpu.make_async_copy(mixed_rows.at[:, lanes[k]], out.at[:, lanes[k]], emit_sem.at[k])

    for k in range(3):
        lo, hi = cols[k]
        total = dense[:, lo:hi]
        for d in beside:
            partial(k, d).wait_recv()
            total = total + rs_in[d, :, lo:hi].astype(F32)
        mixed_rows[:, lo:hi] = total.astype(BF16)
        emit(k).start()

    for k in range(3):
        for d in ring:
            tell(k, d).wait_send()
        for i in range(2):
            share_tokens(k, beside[i]).wait_send()
            pass_on(k, i).wait_send()
            fold(k, i).wait_send()
            partial(k, beside[i]).wait_send()
        for e in range(cores):
            blocks = len(of_core[e]) * (side - 1)
            bulk(send, k, blocks, out_send.at[1 + e, k], out_recv.at[1 + e, k]).wait_send()
        bulk(send, k, peers, out_send.at[0, k], out_recv.at[0, k]).wait_send()
        for group in range(2):
            blocks = peers * (1 if group == 0 else side - 1)
            bulk(result, k, blocks, ret_send.at[group, k], ret_recv.at[group, k]).wait_send()
    for stage in range(4):
        leave(stage)
    for p in range(4):
        for i in range(2):
            piece_on(p, i, False).wait_send()
    for k in range(3):
        emit(k).wait()


def on_device(tokens, norm_gain, route_ids, route_weight, expert_gate, expert_up, expert_down, dense_up, dense_down, branch_gate):
    n = lax.axis_size("ep")
    assert expert_gate.shape[0] == 1
    rows, width = tokens.shape
    ff = expert_gate.shape[2]
    d_rows, dh = dense_up.shape
    cores = 2
    side = round((n // cores) ** (1 / 3))
    assert side == 4 and side ** 3 * cores == n
    tile = width // 128
    cuts = [tile // 3, tile // 3 * 2, tile]
    cols = tuple((lo * 128, hi * 128) for lo, hi in zip([0, *cuts[:2]], cuts))
    plane = n // side
    vmem = pl.BlockSpec(memory_space=pltpu.VMEM)
    hbm = pl.BlockSpec(memory_space=pl.ANY)
    dma = pltpu.SemaphoreType.DMA
    return pl.pallas_call(
        functools.partial(kernel, side, cores, cols),
        out_shape=jax.ShapeDtypeStruct((rows, width), BF16),
        in_specs=[vmem, vmem, vmem, vmem, hbm, hbm, hbm, hbm, hbm, vmem],
        out_specs=hbm,
        scratch_shapes=[
            pltpu.VMEM((side, rows, width), BF16),
            pltpu.VMEM((8, rows), F32),
            pltpu.VMEM((3, side, 8, rows), F32),
            pltpu.VMEM((n, CAP, width), BF16),
            pltpu.VMEM((n, CAP, width), BF16),
            pltpu.VMEM((n, CAP, width), BF16),
            pltpu.VMEM((n, CAP, width), BF16),
            pltpu.VMEM((side, rows, width), BF16),
            pltpu.VMEM((side, rows, width), BF16),
            pltpu.VMEM((2, rows // 2, width), BF16),
            pltpu.VMEM((3, side, 2 * rows, plane * CAP), BF16),
            pltpu.VMEM((rows, width), F32),
            pltpu.VMEM((rows, width), BF16),
            pltpu.VMEM((width, ff), BF16),
            pltpu.VMEM((width, ff), BF16),
            pltpu.VMEM((ff, width), BF16),
            pltpu.VMEM((2, side, side, side, cores, d_rows, dh), BF16),
            pltpu.SemaphoreType.REGULAR,
            dma((5,)), dma((3, side)), dma((3, side)), dma((3, side)), dma((3, side)),
            dma((1 + cores, 3)), dma((1 + cores, 3)), dma((4, 3)),
            dma((2, 3)), dma((2, 3)), dma((3, side)), dma((3, side)),
            dma((4, 4, side)), dma((4, 4, side)),
            dma((3, 2)), dma((3, 2)), dma((3, 2)), dma((3, 2)), dma((4, 2)), dma((4, 2)), dma((3,)),
        ],
        compiler_params=pltpu.CompilerParams(
            collective_id=0, has_side_effects=True, vmem_limit_bytes=62 * 1024 * 1024
        ),
    )(
        tokens, norm_gain.reshape(1, -1), route_ids.T, route_weight.T,
        expert_gate, expert_up, expert_down, dense_up, dense_down.T, branch_gate.reshape(1, -1),
    )


def solution(mesh):
    placed = (
        P("ep", None), P(), P("ep", None), P("ep", None),
        P("ep", None, None), P("ep", None, None), P("ep", None, None),
        P("ep", None), P(None, "ep"), P(),
    )
    return jax.shard_map(
        on_device, mesh=mesh, in_specs=placed, out_specs=P("ep", None), check_vma=False
    )
```

```python
import functools
import itertools
import math

import jax
import jax.numpy as jnp
from jax import lax
from jax.experimental import pallas as pl
from jax.experimental.pallas import tpu as pltpu
from jax.sharding import PartitionSpec as P

CAP = 8
F32 = jnp.float32
BF16 = jnp.bfloat16


def plane_order(side, cores):
    def hop(d):
        return min(d, side - d)

    offsets = [o for o in itertools.product(range(side), range(side), range(cores)) if any(o)]
    order = []
    for o in sorted(offsets, key=lambda o: hop(o[0]) + hop(o[1])):
        for pick in (o, (-o[0] % side, -o[1] % side, o[2])):
            if pick not in order:
                order.append(pick)
    return order


def with_dim(k, d, a, b, e):
    full = [a, b]
    full.insert(k, d)
    return (*full, e)


def kernel(
    side, cores, cols,
    tokens, gain, ids, weight, w_gate, w_up, w_down, d_up, d_down, branch,
    out,
    ag, mine, info, send, recv, result, back, rs_out, rs_in, folded, shares, dense, mixed_rows, v_gate, v_up, v_down, wide,
    ready, local_sem, info_send, info_recv, ag_send, ag_recv, out_send, out_recv, own_sem,
    ret_send, ret_recv, rs_send, rs_recv, w_send, w_recv,
    pass_send, pass_recv, fold_send, fold_recv, on_send, on_recv, emit_sem,
):
    rows, width = tokens.shape
    plane = side * side * cores
    n = side * plane
    slots = plane * CAP
    me = lax.axis_index("ep")
    dims = (side, side, side, cores)
    strides = (plane, side * cores, cores, 1)
    at = tuple(me // strides[i] % dims[i] for i in range(4))
    part = [[(at[i] + d) % dims[i] * strides[i] for d in range(dims[i])] for i in range(4)]
    grid = (side, side, side, cores, CAP, width)
    by_core = (cores, side, side, side, CAP, width)
    send6, back6 = (r.reshape(*grid) for r in (send, back))
    recv6, result6 = (r.reshape(*by_core) for r in (recv, result))
    ring = sorted(range(1, side), key=lambda d: (min(d, side - d), d))
    others = pl.ds(1, side - 1)
    order = plane_order(side, cores)
    peers = len(order)
    of_core = [[o for o in order if o[2] == e] for e in range(cores)]
    lanes = [pl.ds(lo, hi - lo) for lo, hi in cols]

    def dev(o):
        return part[0][o[0]] + part[1][o[1]] + part[2][o[2]] + part[3][o[3]]

    def minus(o):
        return tuple(-o[i] % dims[i] for i in range(4))

    def along(k, d):
        return tuple(d if i == k else 0 for i in range(4))

    def remote(src, dst, s, r, target):
        return pltpu.make_async_remote_copy(
            src_ref=src, dst_ref=dst, send_sem=s, recv_sem=r,
            device_id=(target,), device_id_type=pl.DeviceIdType.MESH,
        )

    near = dev((0, 0, 0, 1))

    barrier = pltpu.get_barrier_semaphore()
    line = [along(k, d) for d in ring for k in range(3)]
    greeted = line + [(*o[:3], 1) for o in line] + [(0, 0, 0, 1)]

    def greet(semaphore, offsets):
        for o in offsets:
            pl.semaphore_signal(semaphore, inc=1, device_id=(dev(o),), device_id_type=pl.DeviceIdType.MESH)

    greet(barrier, greeted)

    own_up = pltpu.make_async_copy(d_up, wide.at[(0, *at)], local_sem.at[0])
    own_down = pltpu.make_async_copy(d_down, wide.at[(1, *at)], local_sem.at[1])
    own_up.start()
    own_down.start()
    loads = [
        pltpu.make_async_copy(w_gate.at[0], v_gate, local_sem.at[2]),
        pltpu.make_async_copy(w_up.at[0], v_up, local_sem.at[3]),
        pltpu.make_async_copy(w_down.at[0], v_down, local_sem.at[4]),
    ]
    for load in loads:
        load.start()

    x = tokens[...].astype(F32)
    scale = lax.rsqrt(jnp.mean(x * x, axis=-1, keepdims=True) + 1e-06)
    ag[0] = (x * scale * gain[...]).astype(BF16)
    mine[...] = jnp.concatenate(
        [ids[...].astype(F32), weight[...], jnp.zeros((4, rows), F32)], axis=0
    )

    before = lax.broadcasted_iota(jnp.int32, (rows, rows), 0) < lax.broadcasted_iota(jnp.int32, (rows, rows), 1)
    before = before.astype(F32).astype(BF16)
    j_iota = lax.broadcasted_iota(jnp.int32, (plane, rows), 0)
    p_iota = lax.broadcasted_iota(jnp.int32, (slots, rows), 0)

    def slots_of(k, facts):
        first, second = [i for i in range(3) if i != k]

        def local(expert):
            coords = [expert // strides[i] % dims[i] for i in range(4)]
            away = [(coords[i] + dims[i] - at[i]) % dims[i] for i in range(4)]
            j = (away[first] * side + away[second]) * cores + away[3]
            return jnp.where(away[k] == 0, j, -1)

        j0 = local(facts[0:1, :].astype(jnp.int32))
        j1 = local(facts[1:2, :].astype(jnp.int32))
        hot0 = (j0 == j_iota).astype(F32)
        hot1 = (j1 == j_iota).astype(F32)
        count = jnp.dot((hot0 + hot1).astype(BF16), before, preferred_element_type=F32)
        rank0 = jnp.sum(hot0 * count, axis=0, keepdims=True).astype(jnp.int32)
        rank1 = jnp.sum(hot1 * count, axis=0, keepdims=True).astype(jnp.int32)
        slot0 = jnp.where(j0 < 0, -1, j0 * CAP + rank0)
        slot1 = jnp.where(j1 < 0, -1, j1 * CAP + rank1)
        return slot0 == p_iota, slot1 == p_iota

    def pack(k, d, facts):
        lo, hi = cols[k]
        table0, table1 = slots_of(k, facts)
        place = jnp.where(table0 | table1, 1.0, 0.0).astype(BF16)
        packed = jnp.dot(place, ag[d, :, lo:hi], preferred_element_type=F32)
        send[d * plane:(d + 1) * plane, :, lo:hi] = packed.reshape(plane, CAP, hi - lo).astype(BF16)
        share = jnp.where(table0, facts[2:3, :], 0.0) + jnp.where(table1, facts[3:4, :], 0.0)
        share = share.T
        high = share.astype(BF16)
        shares[k, d, :rows] = high
        shares[k, d, rows:] = (share - high.astype(F32)).astype(BF16)

    def core_first(o):
        return (o[3], *o[:3])

    def sources(k, group, j):
        return core_first(with_dim(k, 0 if group == 0 else others, *j))

    def slot_rows(group, j):
        return (0 if group == 0 else others, *j)

    def dispatch(k, group, d, j):
        return remote(
            send6.at[(d, *j, slice(None), lanes[k])],
            recv6.at[(*core_first(with_dim(k, d, *j)), slice(None), lanes[k])],
            out_send.at[group, k], out_recv.at[group, k], dev(with_dim(k, 0, *j)),
        )

    here = (0, 0, 0)

    def keep(k, group):
        return pltpu.make_async_copy(
            send6.at[(*slot_rows(group, here), slice(None), lanes[k])],
            recv6.at[(*sources(k, group, here), slice(None), lanes[k])],
            own_sem.at[group, k],
        )

    def turns(targets):
        count = len(targets)
        return [(k, targets[(i + k * count // 3) % count]) for i in range(count) for k in range(3)]

    def start_own(e):
        for k, j in turns(of_core[e]):
            dispatch(k, 0, 0, j).start()

    def start_ring(e):
        def round_of(d, carry):
            for k, j in turns(of_core[e]):
                dispatch(k, 1 + e, d, j).start()
            return carry

        lax.fori_loop(1, side, round_of, 0)

    def bulk(buffer, k, blocks, s, r):
        part_of = buffer.at[pl.ds(0, blocks), :, lanes[k]]
        return remote(part_of, part_of, s, r, near)

    for k in range(3):
        pack(k, 0, mine)

    own_up.wait()
    own_down.wait()
    pl.semaphore_wait(barrier, len(greeted))
    greet(ready, line)

    def tell(k, d):
        return remote(mine, info.at[k, d], info_send.at[k, d], info_recv.at[k, d], dev(along(k, d)))

    def share_tokens(k, d):
        return remote(
            ag.at[0, :, lanes[k]], ag.at[d, :, lanes[k]], ag_send.at[k, d], ag_recv.at[k, d], dev(along(k, d))
        )

    for d in ring:
        for k in range(3):
            tell(k, d).start()
    half = rows // 2
    beside = (1, side - 1)

    def pass_on(k, i):
        d = beside[i]
        part_of = pl.ds(i * half, half)
        return remote(
            ag.at[d, part_of, lanes[k]], ag.at[2, part_of, lanes[k]],
            pass_send.at[k, i], pass_recv.at[k, i], dev(along(k, d)),
        )

    for d in beside:
        for k in range(3):
            share_tokens(k, d).start()

    pieces = (
        (0, 0, 256, (0, 1, 2, 3)),
        (0, 256, 512, (1, 0, 2, 3)),
        (1, 0, 256, (1, 2, 0, 3)),
        (1, 256, 512, (2, 0, 1, 3)),
    )

    def piece_copy(p, stage, d, incoming):
        which, lo, hi, turn = pieces[p]
        axis = turn[stage]
        where = list(at)
        for held in turn[:stage]:
            where[held] = slice(None)
        if incoming:
            where[axis] = (at[axis] + dims[axis] - d) % dims[axis]
        block = wide.at[(which, *where, slice(None), pl.ds(lo, hi - lo))]
        offset = along(axis, d)
        return remote(block, block, w_send.at[p, stage, d], w_recv.at[p, stage, d], dev(offset))

    def each(stage, act, incoming=False):
        for p in range(4):
            axis = pieces[p][3][stage]
            for d in beside if stage == 2 else range(1, dims[axis]):
                act(piece_copy(p, stage, d, incoming))

    def piece_on(p, i, incoming):
        which, lo, hi, turn = pieces[p]
        axis = turn[2]
        where = list(at)
        where[turn[0]] = pl.ds(i * (side // 2), side // 2)
        where[turn[1]] = slice(None)
        where[axis] = (at[axis] + side - (2 if incoming else beside[i])) % side
        block = wide.at[(which, *where, slice(None), pl.ds(lo, hi - lo))]
        return remote(block, block, on_send.at[p, i], on_recv.at[p, i], dev(along(axis, beside[i])))

    def begin(stage):
        each(stage, lambda copy: copy.start())

    def arrive(stage):
        each(stage, lambda copy: copy.wait_recv(), True)

    def leave(stage):
        each(stage, lambda copy: copy.wait_send())

    begin(0)
    pl.semaphore_wait(ready, len(line))
    start_own(0)

    for i in range(2):
        for k in range(3):
            share_tokens(k, beside[i]).wait_recv()
            pass_on(k, i).start()
    start_own(1)
    for d in beside:
        for k in range(3):
            tell(k, d).wait_recv()
            pack(k, d, info[k, d])
    arrive(0)
    begin(1)
    for k in range(3):
        keep(k, 0).start()
        tell(k, 2).wait_recv()
        for i in range(2):
            pass_on(k, i).wait_recv()
        pack(k, 2, info[k, 2])
    start_ring(0)
    arrive(1)
    begin(2)
    start_ring(1)
    for k in range(3):
        keep(k, 1).start()

    for load in loads:
        load.wait()

    part_rows = n // (2 * cores)

    def experts_on(p):
        block = pl.ds(p * part_rows, part_rows)
        x_in = recv[block].reshape(part_rows * CAP, width)
        gate_part = jnp.dot(x_in, v_gate[...], preferred_element_type=F32)
        up_part = jnp.dot(x_in, v_up[...], preferred_element_type=F32)
        hidden = (gate_part / (1.0 + jnp.exp(-gate_part)) * up_part).astype(BF16)
        res = jnp.dot(hidden, v_down[...], preferred_element_type=F32)
        result[block] = res.reshape(part_rows, CAP, width).astype(BF16)

    def giveback(k, group, d, j):
        return remote(
            result6.at[(*core_first(with_dim(k, d, *j)), slice(None), lanes[k])],
            back6.at[(d, *j, slice(None), lanes[k])],
            ret_send.at[group, k], ret_recv.at[group, k], dev(minus(with_dim(k, 0, *j))),
        )

    def keep_back(k, group):
        d = others if group else 0
        return pltpu.make_async_copy(
            result6.at[(*core_first(with_dim(k, d, *here)), slice(None), lanes[k])],
            back6.at[(d, *here, slice(None), lanes[k])], own_sem.at[2 + group, k],
        )

    def wait_group(group, k, blocks):
        bulk(recv, k, blocks, out_send.at[group, k], out_recv.at[group, k]).wait_recv()

    def back_own(e):
        for k, j in turns(of_core[e]):
            giveback(k, 0, 0, j).start()

    def back_ring(e):
        def round_of(d, carry):
            for k, j in turns(of_core[e]):
                giveback(k, 1, d, j).start()
            return carry

        lax.fori_loop(1, side, round_of, 0)

    for e in range(cores):
        for k in range(3):
            if e == 0:
                keep(k, 0).wait()
                keep(k, 1).wait()
                wait_group(0, k, peers)
            wait_group(1 + e, k, len(of_core[e]) * (side - 1))
        for p in range(2):
            experts_on(e * 2 + p)
        back_ring(e)
    arrive(2)
    for p in range(4):
        for i in range(2):
            piece_on(p, i, False).start()
    back_own(0)
    for k in range(3):
        keep_back(k, 1).start()
        keep_back(k, 0).start()

    def combine(k, d):
        lo, hi = cols[k]
        rows_back = back[d * plane:(d + 1) * plane, :, lo:hi].reshape(slots, hi - lo)
        total = jnp.dot(shares[k, d], rows_back, preferred_element_type=F32)
        return total[:rows] + total[rows:]

    def partial(k, d):
        return remote(
            rs_out.at[d, :, lanes[k]], rs_in.at[d, :, lanes[k]], rs_send.at[k, d], rs_recv.at[k, d],
            dev(along(k, -d % side)),
        )

    def fold(k, i):
        part_of = pl.ds(i * half, half)
        return remote(
            rs_out.at[2, part_of, lanes[k]], folded.at[i, :, lanes[k]],
            fold_send.at[k, i], fold_recv.at[k, i], dev(along(k, -beside[i] % side)),
        )

    for k in range(3):
        lo, hi = cols[k]
        keep_back(k, 1).wait()
        bulk(back, k, peers * (side - 1), ret_send.at[1, k], ret_recv.at[1, k]).wait_recv()
        rs_out[2, :, lo:hi] = combine(k, 2).astype(BF16)
        for i in range(2):
            fold(k, i).start()
    back_own(1)
    for p in range(4):
        for i in range(2):
            piece_on(p, i, True).wait_recv()
    begin(3)
    for k in range(3):
        lo, hi = cols[k]
        for i in range(2):
            total = combine(k, beside[i])
            fold(k, i).wait_recv()
            mixed = total[i * half:(i + 1) * half] + folded[i, :, lo:hi].astype(F32)
            rest = total[(1 - i) * half:(2 - i) * half]
            rs_out[beside[i], i * half:(i + 1) * half, lo:hi] = mixed.astype(BF16)
            rs_out[beside[i], (1 - i) * half:(2 - i) * half, lo:hi] = rest.astype(BF16)
            partial(k, beside[i]).start()

    arrive(3)
    dense_pre = jnp.dot(ag[0], wide[0].reshape(width, -1), preferred_element_type=F32)
    dense_hidden = (dense_pre / (1.0 + jnp.exp(-dense_pre))).astype(BF16)
    dense_out = lax.dot_general(
        dense_hidden, wide[1].reshape(width, -1), (((1,), (1,)), ((), ())), preferred_element_type=F32
    )
    dense[...] = jnp.tanh(branch[...]) * dense_out
    for k in range(3):
        lo, hi = cols[k]
        keep_back(k, 0).wait()
        bulk(back, k, peers, ret_send.at[0, k], ret_recv.at[0, k]).wait_recv()
        dense[:, lo:hi] += combine(k, 0)

    def emit(k):
        return pltpu.make_async_copy(mixed_rows.at[:, lanes[k]], out.at[:, lanes[k]], emit_sem.at[k])

    for k in range(3):
        lo, hi = cols[k]
        total = dense[:, lo:hi]
        for d in beside:
            partial(k, d).wait_recv()
            total = total + rs_in[d, :, lo:hi].astype(F32)
        mixed_rows[:, lo:hi] = total.astype(BF16)
        emit(k).start()

    for k in range(3):
        for d in ring:
            tell(k, d).wait_send()
        for i in range(2):
            share_tokens(k, beside[i]).wait_send()
            pass_on(k, i).wait_send()
            fold(k, i).wait_send()
            partial(k, beside[i]).wait_send()
        for e in range(cores):
            blocks = len(of_core[e]) * (side - 1)
            bulk(send, k, blocks, out_send.at[1 + e, k], out_recv.at[1 + e, k]).wait_send()
        bulk(send, k, peers, out_send.at[0, k], out_recv.at[0, k]).wait_send()
        for group in range(2):
            blocks = peers * (1 if group == 0 else side - 1)
            bulk(result, k, blocks, ret_send.at[group, k], ret_recv.at[group, k]).wait_send()
    for stage in range(4):
        leave(stage)
    for p in range(4):
        for i in range(2):
            piece_on(p, i, False).wait_send()
    for k in range(3):
        emit(k).wait()


def on_device(tokens, norm_gain, route_ids, route_weight, expert_gate, expert_up, expert_down, dense_up, dense_down, branch_gate):
    n = lax.axis_size("ep")
    assert expert_gate.shape[0] == 1
    rows, width = tokens.shape
    ff = expert_gate.shape[2]
    d_rows, dh = dense_up.shape
    cores = 2
    side = round((n // cores) ** (1 / 3))
    assert side == 4 and side ** 3 * cores == n
    tile = width // 128
    cuts = [tile // 3, tile // 3 * 2, tile]
    cols = tuple((lo * 128, hi * 128) for lo, hi in zip([0, *cuts[:2]], cuts))
    plane = n // side
    vmem = pl.BlockSpec(memory_space=pltpu.VMEM)
    hbm = pl.BlockSpec(memory_space=pl.ANY)
    dma = pltpu.SemaphoreType.DMA
    return pl.pallas_call(
        functools.partial(kernel, side, cores, cols),
        out_shape=jax.ShapeDtypeStruct((rows, width), BF16),
        in_specs=[vmem, vmem, vmem, vmem, hbm, hbm, hbm, hbm, hbm, vmem],
        out_specs=hbm,
        scratch_shapes=[
            pltpu.VMEM((side, rows, width), BF16),
            pltpu.VMEM((8, rows), F32),
            pltpu.VMEM((3, side, 8, rows), F32),
            pltpu.VMEM((n, CAP, width), BF16),
            pltpu.VMEM((n, CAP, width), BF16),
            pltpu.VMEM((n, CAP, width), BF16),
            pltpu.VMEM((n, CAP, width), BF16),
            pltpu.VMEM((side, rows, width), BF16),
            pltpu.VMEM((side, rows, width), BF16),
            pltpu.VMEM((2, rows // 2, width), BF16),
            pltpu.VMEM((3, side, 2 * rows, plane * CAP), BF16),
            pltpu.VMEM((rows, width), F32),
            pltpu.VMEM((rows, width), BF16),
            pltpu.VMEM((width, ff), BF16),
            pltpu.VMEM((width, ff), BF16),
            pltpu.VMEM((ff, width), BF16),
            pltpu.VMEM((2, side, side, side, cores, d_rows, dh), BF16),
            pltpu.SemaphoreType.REGULAR,
            dma((5,)), dma((3, side)), dma((3, side)), dma((3, side)), dma((3, side)),
            dma((1 + cores, 3)), dma((1 + cores, 3)), dma((4, 3)),
            dma((2, 3)), dma((2, 3)), dma((3, side)), dma((3, side)),
            dma((4, 4, side)), dma((4, 4, side)),
            dma((3, 2)), dma((3, 2)), dma((3, 2)), dma((3, 2)), dma((4, 2)), dma((4, 2)), dma((3,)),
        ],
        compiler_params=pltpu.CompilerParams(
            collective_id=0, has_side_effects=True, vmem_limit_bytes=62 * 1024 * 1024
        ),
    )(
        tokens, norm_gain.reshape(1, -1), route_ids.T, route_weight.T,
        expert_gate, expert_up, expert_down, dense_up, dense_down.T, branch_gate.reshape(1, -1),
    )


def solution(mesh):
    placed = (
        P("ep", None), P(), P("ep", None), P("ep", None),
        P("ep", None, None), P("ep", None, None), P("ep", None, None),
        P("ep", None), P(None, "ep"), P(),
    )
    return jax.shard_map(
        on_device, mesh=mesh, in_specs=placed, out_specs=P("ep", None), check_vma=False
    )
```
